32 devices in a mesh: sp: 4 (over y, core), tp: 8 (over z, x).
Axes of the slice: x: 2, y: 2, z: 4, core: 2. Of those that a mesh axis runs over, the one named last changes fastest.
Arguments:
- queries: bfloat16 [512, 3072], P('sp'), may hold values from -6 to 6
- attn_out: bfloat16 [512, 3072], P('sp'), may hold values from -3 to 3
- log_norm: float32 [512, 12], P('sp'), as said below
- cotangent: bfloat16 [512, 3072], P('sp'), may hold values from -96 to 96
- keys: bfloat16 [1024, 512], P(('sp', 'tp')), may hold values from -6 to 6
- values: bfloat16 [1024, 512], P(('sp', 'tp')), may hold values from -6 to 6
- source: bfloat16 [1024, 3072], P('sp', 'tp'), may hold values from -6 to 6
- w_query: bfloat16 [3072, 3072], P('tp'), may hold values from -0.109375 to 0.109375
- w_key: bfloat16 [3072, 512], P('tp'), may hold values from -0.109375 to 0.109375
- w_value: bfloat16 [3072, 512], P('tp'), may hold values from -0.109375 to 0.109375
Outputs:
- d_target: bfloat16 [512, 3072], P('sp', 'tp')
- d_source: bfloat16 [1024, 3072], P('sp', 'tp')
- d_wvalue: float32 [3072, 512], P('tp')
The draws below stay inside these ranges and needn't reach their ends.
Inputs may be any that keep to these rules, and one draw needn't show every extreme that they name: `log_norm`: the logarithm of the softmax total saved by the forward pass, near log(1024) + 0.5.
All inputs are finite; a program needn't handle non-finite values.
Results may differ from the reference program's by a relative error of at most 0.024.
Values may be sent and summed in bfloat16 or wider, within the bound.
A program may use at most 64 MiB of HBM per device.

```python
import math
import jax
import jax.numpy as jnp
from jax import lax

HEADS = 12
KV_HEADS = 2
HEAD_DIM = 256
TARGET_ROWS_EACH = 128
D = 3072
KW = 512
TGT = 512
SRC = 1024


def draw_log_norm(key, part):
    center = math.log(SRC) + 0.5
    spread = jax.random.uniform(key, (TGT, HEADS), jnp.float32, -0.5, 0.5)
    return (center + spread).astype(jnp.float32)


def level_of(key, dims, cuts, low, largest):
    def one(dim, blocks):
        heights = jax.random.uniform(jax.random.fold_in(jax.random.fold_in(key, 6), dim), (blocks,), jnp.float32, low / len(cuts), largest / len(cuts))
        return jnp.repeat(jnp.exp(heights), dims[dim] // blocks).reshape((-1,) + (1,) * (len(dims) - dim - 1))

    level = one(*cuts[0])
    for cut in cuts[1:]:
        level = level * one(*cut)
    return level


def scatter_about(own_key, extent, deviation, limit, shards=(), kind=jnp.bfloat16):
    factor_of = level_of(own_key, extent, shards, -0.22, 0.18) if shards else 1.0
    values = jax.random.normal(own_key, extent, jnp.float32) * deviation * factor_of
    return jnp.minimum(jnp.maximum(values, -limit), limit).astype(kind)


def setup_inputs(seed: int = 0) -> dict:
    splits = jax.random.split(jax.random.key(seed), 11)
    return {
        "queries": scatter_about(splits[0], (TGT, D), 1.0, 6.0, ((0, 4),)),
        "attn_out": scatter_about(splits[1], (TGT, D), 0.5, 3.0, ((0, 4),)),
        "log_norm": draw_log_norm(jax.random.fold_in(splits[10], 71), 0),
        "cotangent": scatter_about(splits[3], (TGT, D), 16.0, 96.0, ((0, 4),)),
        "keys": scatter_about(splits[4], (SRC, KW), 1.0, 6.0, ((0, 32),)),
        "values": scatter_about(splits[5], (SRC, KW), 1.0, 6.0, ((0, 32),)),
        "source": scatter_about(splits[6], (SRC, D), 1.0, 6.0, ((0, 4), (1, 8))),
        "w_query": scatter_about(splits[7], (D, D), D ** -0.5, 0.109375, ((0, 8),)),
        "w_key": scatter_about(splits[8], (D, KW), D ** -0.5, 0.109375, ((0, 8),)),
        "w_value": scatter_about(splits[9], (D, KW), D ** -0.5, 0.109375, ((0, 8),)),
    }


def reference(queries, attn_out, log_norm, cotangent, keys, values, source, w_query, w_key, w_value):
    single_precision = jnp.float32
    repeat = HEADS // KV_HEADS
    score_scale = 1.0 / math.sqrt(HEAD_DIM)
    src_rows = keys.shape[0]
    shared_key_heads = keys.astype(single_precision).reshape(src_rows, KV_HEADS, HEAD_DIM)
    shared_value_heads = values.astype(single_precision).reshape(src_rows, KV_HEADS, HEAD_DIM)
    blocks = queries.shape[0] // TARGET_ROWS_EACH

    def step(carry, index):
        dk_total, dv_total = carry
        start = index * TARGET_ROWS_EACH

        def rows(array):
            return lax.dynamic_slice_in_dim(array, start, TARGET_ROWS_EACH, 0)
        query_tensor4 = rows(queries).astype(single_precision).reshape(TARGET_ROWS_EACH, KV_HEADS, repeat, HEAD_DIM)
        output_gradient4 = rows(cotangent).astype(single_precision).reshape(TARGET_ROWS_EACH, KV_HEADS, repeat, HEAD_DIM)
        out4 = rows(attn_out).astype(single_precision).reshape(TARGET_ROWS_EACH, KV_HEADS, repeat, HEAD_DIM)
        lse = jnp.transpose(rows(log_norm).reshape(TARGET_ROWS_EACH, KV_HEADS, repeat), (1, 2, 0))[..., None]
        delta = jnp.transpose(lax.optimization_barrier(jnp.sum(output_gradient4 * out4, axis=3)), (1, 2, 0))[..., None]
        logit_scores = jnp.einsum('znjk,wnk->njzw', query_tensor4, shared_key_heads) * score_scale
        probs = jnp.exp(logit_scores - lse)
        probabilities16 = lax.optimization_barrier(probs.astype(jnp.bfloat16)).astype(single_precision)
        prob_gradient = jnp.einsum('znjk,wnk->njzw', output_gradient4, shared_value_heads)
        score_gradient = lax.optimization_barrier((probs * (prob_gradient - delta)).astype(jnp.bfloat16)).astype(single_precision)
        query_gradient = (jnp.einsum('wohn,nwb->hwob', score_gradient, shared_key_heads) * score_scale).reshape(TARGET_ROWS_EACH, -1)
        key_gradient = jnp.einsum('nkjv,jnka->vna', score_gradient, query_tensor4) * score_scale
        value_gradient = jnp.einsum('nkjv,jnka->vna', probabilities16, output_gradient4)
        dk16 = lax.optimization_barrier(key_gradient.reshape(src_rows, -1).astype(jnp.bfloat16)).astype(single_precision)
        dv16 = lax.optimization_barrier(value_gradient.reshape(src_rows, -1).astype(jnp.bfloat16)).astype(single_precision)
        return ((dk_total + dk16, dv_total + dv16), query_gradient.astype(jnp.bfloat16))
    start_carry = (jnp.zeros((src_rows, KW), single_precision), jnp.zeros((src_rows, KW), single_precision))
    (dk_total, dv_total), dq_blocks = lax.scan(step, start_carry, jnp.arange(blocks, dtype=jnp.int32))
    dq16 = dq_blocks.reshape(queries.shape[0], -1)
    d_target = jnp.dot(dq16, w_query.T, preferred_element_type=single_precision).astype(jnp.bfloat16)
    stacked = jnp.concatenate([dk_total.astype(jnp.bfloat16), dv_total.astype(jnp.bfloat16)], axis=1)
    weights = jnp.concatenate([w_key, w_value], axis=1)
    d_source = jnp.dot(stacked, weights.T, preferred_element_type=single_precision).astype(jnp.bfloat16)
    d_wvalue = jnp.dot(source.T, dv_total.astype(jnp.bfloat16), preferred_element_type=single_precision)
    return (d_target, d_source, d_wvalue)
```

```python
import functools
import math

import jax
import jax.numpy as jnp
from jax import lax
from jax.experimental import pallas as pl
from jax.experimental.pallas import tpu as pltpu
from jax.sharding import PartitionSpec as P

HEADS = 12
KV_HEADS = 2
HEAD_DIM = 256
CORES = 2
SIDE = 2
VMEM_BYTES = 60 * 1024 * 1024
MESH = pl.DeviceIdType.MESH
NT = (((1,), (1,)), ((), ()))
TN = (((0,), (0,)), ((), ()))
F32 = jnp.float32
BF16 = jnp.bfloat16


def dot(a, b, dims=(((1,), (0,)), ((), ()))):
    return lax.dot_general(a, b, dims, preferred_element_type=F32)


def kernel(
    sp, tp, lse_ref, k_ref, v_ref, q_hbm, o_hbm, do_hbm, src_hbm, wq_hbm, wk_hbm, wv_hbm,
    dt_ref, ds_ref, dw_ref,
    kv, qs, dos, os_, wq, wk, wv, src, src_t, lse, delta, dqa, dq16, part, got, full,
    load_sem, near_send, near_recv, kv_send, kv_recv, kv_pair_send, kv_pair_recv,
    src_send, src_recv, part_send, part_recv, g_send, g_recv, gy_send, gy_recv, gp_send, gp_recv, kvz_send, gz_send,
):
    rows = q_hbm.shape[0]
    rs, kw = k_ref.shape
    repeat = HEADS // KV_HEADS
    scale = 1.0 / math.sqrt(HEAD_DIM)
    i, j = lax.axis_index("sp"), lax.axis_index("tp")
    ny, nz = sp // CORES, tp // SIDE
    y, c = i // CORES, lax.rem(i, CORES)
    z, x = j // SIDE, lax.rem(j, SIDE)
    sp_peers = [lax.rem(i + k, sp) for k in range(1, sp)]
    y_peers = [lax.rem(y + k, ny) * CORES + c for k in range(1, ny)]
    pair = y * CORES + 1 - c
    orders = [sorted((b for b in range(nz) if b != a), key=lambda b, a=a: abs(a - b)) for a in range(nz)]
    zs = [sum(jnp.where(z == a, order[n], 0) for a, order in enumerate(orders)) for n in range(nz - 1)]
    onward = [jnp.where(a > z, z - 1, z + 1) for a in zs]
    onward_ok = [(b >= 0) & (b < nz) for b in onward]
    z_peers = [a * SIDE + x for a in zs]
    jx = z * SIDE + 1 - x
    sends = []
    maybe_sends = []

    def send_if(condition, make):
        pl.when(condition)(lambda: make().start())
        maybe_sends.append((condition, make))

    def along_z(ref, n, s, r):
        targets = [(z + 1, z + 1 < nz, 0), (z - 1, z >= 1, 1)] if n is None else [(onward[n], onward_ok[n], n + 2)]
        for to, ok, at in targets:
            send_if(ok, lambda to=to, at=at: pltpu.make_async_remote_copy(
                src_ref=ref, dst_ref=ref, send_sem=s.at[at], recv_sem=r,
                device_id=(i, to * SIDE + x), device_id_type=MESH,
            ))

    def send(ref_from, ref_to, s, r, device):
        copy = pltpu.make_async_remote_copy(
            src_ref=ref_from, dst_ref=ref_to, send_sem=s, recv_sem=r,
            device_id=device, device_id_type=MESH,
        )
        copy.start()
        sends.append(copy)

    def receive(ref, r):
        pltpu.make_async_remote_copy(
            src_ref=ref, dst_ref=ref, send_sem=load_sem.at[0], recv_sem=r,
            device_id=(pair, j), device_id_type=MESH,
        ).wait_recv()

    loads = []

    def load(ref_from, ref_to):
        copy = pltpu.make_async_copy(ref_from, ref_to, load_sem.at[len(loads)])
        copy.start()
        loads.append(copy)
        return copy

    barrier = pltpu.get_barrier_semaphore()
    near = [(p, j) for p in sp_peers] + [(i, p) for p in z_peers] + [(i, jx)]
    for d in near:
        pl.semaphore_signal(barrier, inc=1, device_id=d, device_id_type=MESH)
    near_rows = pl.ds(pl.multiple_of(i * rs, rs), rs)
    own_copies = [load(r, kv.at[t, j, near_rows]) for t, r in enumerate((k_ref, v_ref))]
    attn_loads = []
    for g in range(KV_HEADS):
        for h in range(repeat):
            columns = pl.ds((g * repeat + h) * HEAD_DIM, HEAD_DIM)
            for a, b in ((q_hbm, qs), (do_hbm, dos), (o_hbm, os_)):
                attn_loads.append(load(a.at[:, columns], b.at[g, pl.ds(h * rows, rows)]))
    src_load = load(src_hbm, src.at[i])
    weight_loads = [load(wq_hbm, wq), load(wk_hbm, wk), load(wv_hbm, wv)]
    pl.semaphore_wait(barrier, len(near))

    for n, p in enumerate(sp_peers):
        for t, r in enumerate((k_ref, v_ref)):
            send(r, kv.at[t, j, near_rows], near_send.at[t, n], near_recv.at[t, i], (p, j))

    for copy in attn_loads:
        copy.wait()
    for g in range(KV_HEADS):
        for h in range(repeat):
            at = pl.ds(h * rows, rows)
            d = jnp.sum(dos[g, at].astype(F32) * os_[g, at].astype(F32), axis=1, keepdims=True)
            delta[g, at] = jnp.broadcast_to(d, (rows, 128))
            n = g * repeat + h
            lse[g, at] = jnp.transpose(jnp.broadcast_to(lse_ref[n:n + 1, :], (128, rows)))

    for copy in own_copies:
        copy.wait()
    for p in sp_peers:
        for t in range(2):
            receive(kv.at[t, j, pl.ds(pl.multiple_of(p * rs, rs), rs)], near_recv.at[t, p])

    def kv_to_x(slot, n):
        send(kv.at[c, slot], kv.at[c, slot], kv_send.at[n], kv_recv.at[slot], (i, jx))

    def kv_to_pair(slot):
        send(kv.at[c, slot], kv.at[c, slot], kv_pair_send.at[slot], kv_pair_recv.at[slot], (pair, j))

    kv_to_x(j, 0)
    along_z(kv.at[c, j], None, kvz_send, kv_recv.at[j])

    def wide(a, n):
        return a if n == 1 else jnp.concatenate([a] * n, axis=1)

    def grads(g, keys, values):
        n = keys.shape[0] // 128
        p = jnp.exp(dot(qs[g], keys, NT) * scale - wide(lse[g], n))
        dp = dot(dos[g], values, NT)
        ds = (p * (dp - wide(delta[g], n))).astype(BF16)
        return p, ds

    def head_columns(g):
        return slice(g * HEAD_DIM, (g + 1) * HEAD_DIM)

    for g in range(KV_HEADS):
        cols = head_columns(g)
        keys = kv[0, j, :, cols]
        p, ds = grads(g, keys, kv[1, j, :, cols])
        dk = dot(ds, qs[g], TN) * scale
        dv = dot(p.astype(BF16), dos[g], TN)
        part[:, 0, :, cols] = dk.astype(BF16).reshape(sp, rs, HEAD_DIM)
        part[:, 1, :, cols] = dv.astype(BF16).reshape(sp, rs, HEAD_DIM)
        dqa[g] = dot(ds, keys)
    for n, p in enumerate(sp_peers):
        send(part.at[p], got.at[i], part_send.at[n], part_recv.at[i], (p, j))
    src_load.wait()
    for n, p in enumerate(y_peers):
        send(src.at[i], src.at[i], src_send.at[n], src_recv.at[i], (p, j))
    send(src.at[i], src.at[i], src_send.at[ny], src_recv.at[i], (pair, j))

    def chunk_one(slot):
        for g in range(KV_HEADS):
            cols = head_columns(g)
            keys = kv[0, slot, :, cols]
            _, ds = grads(g, keys, kv[1, slot, :, cols])
            dqa[g] += dot(ds, keys)

    def chunk_z(a):
        slots = pl.ds(a * SIDE, SIDE)
        for g in range(KV_HEADS):
            cols = head_columns(g)
            keys = kv[0, slots, :, cols].reshape(-1, HEAD_DIM)
            values = kv[1, slots, :, cols].reshape(-1, HEAD_DIM)
            _, ds = grads(g, keys, values)
            dqa[g] += dot(ds, keys)

    def from_z(n):
        slot = z_peers[n]
        receive(kv.at[c, slot], kv_recv.at[slot])
        along_z(kv.at[c, slot], n, kvz_send, kv_recv.at[slot])
        kv_to_x(slot, n + 1)
        kv_to_pair(slot)

    def from_x(slot):
        receive(kv.at[c, slot], kv_recv.at[slot])
        kv_to_pair(slot)

    def from_pair(slot):
        receive(kv.at[1 - c, slot], kv_pair_recv.at[slot])

    def g_to_x(slot, n):
        send(full.at[i, slot], full.at[i, slot], g_send.at[n], g_recv.at[slot], (i, jx))

    def g_spread(slot):
        for n, p in enumerate(y_peers):
            send(full.at[i, slot, 1], full.at[i, slot, 1], gy_send.at[n, slot], gy_recv.at[i, slot], (p, j))
        send(full.at[i, slot, 1], full.at[i, slot, 1], gp_send.at[i, slot], gp_recv.at[i, slot], (pair, j))

    def g_from_z(n):
        slot = z_peers[n]
        receive(full.at[i, slot], g_recv.at[slot])
        along_z(full.at[i, slot], n, gz_send, g_recv.at[slot])
        g_to_x(slot, n + 1)
        g_spread(slot)

    def g_from_x(slot):
        receive(full.at[i, slot], g_recv.at[slot])
        g_spread(slot)

    def g_from_y(slot):
        for p in y_peers:
            receive(full.at[p, slot, 1], gy_recv.at[p, slot])
            send(full.at[p, slot, 1], full.at[p, slot, 1], gp_send.at[p, slot], gp_recv.at[p, slot], (pair, j))

    far = [a * SIDE + 1 - x for a in zs]
    from_x(jx)
    from_z(0)
    total = part[i].astype(F32)
    for p in sp_peers:
        receive(got.at[p], part_recv.at[p])
        total += got[p].astype(F32)
    full[i, j] = total.astype(BF16)
    along_z(full.at[i, j], None, gz_send, g_recv.at[j])
    g_to_x(j, 0)
    g_spread(j)
    from_pair(jx)
    chunk_one(jx)
    for n in range(nz - 1):
        if n + 1 < nz - 1:
            from_z(n + 1)
        from_x(far[n])
        g_from_z(n)
        if n == 0:
            g_from_x(jx)
            for m, p in enumerate(y_peers):
                receive(src.at[p], src_recv.at[p])
                send(src.at[p], src.at[p], src_send.at[ny + 1 + m], src_recv.at[p], (pair, j))
        else:
            g_from_x(far[n - 1])
        g_from_y([j, jx, z_peers[0]][n])
        from_pair(z_peers[n])
        from_pair(far[n])
        chunk_z(zs[n])
    g_from_x(far[nz - 2])
    for copy in weight_loads:
        copy.wait()
    for g in range(KV_HEADS):
        for h in range(repeat):
            n = g * repeat + h
            dq16[:, n * HEAD_DIM:(n + 1) * HEAD_DIM] = (dqa[g, h * rows:(h + 1) * rows] * scale).astype(BF16)
    theirs = [lax.rem(y + k, ny) * CORES + 1 - c for k in range(ny)]
    for p in theirs:
        receive(src.at[p], src_recv.at[p])
    for b in range(sp):
        src_t[b] = jnp.transpose(src[b])
    dt_ref[...] = dot(dq16[...], wq[...], NT).astype(BF16)
    for slot in z_peers[1:] + far:
        g_from_y(slot)
    ds_ref[...] = (
        dot(full[i, :, 0].reshape(-1, kw), wk[...], NT) + dot(full[i, :, 1].reshape(-1, kw), wv[...], NT)
    ).astype(BF16)
    for p in theirs:
        for slot in range(tp):
            receive(full.at[p, slot, 1], gp_recv.at[p, slot])
    dw = dot(src_t[0], full[0, :, 1].reshape(-1, kw))
    for b in range(1, sp):
        dw += dot(src_t[b], full[b, :, 1].reshape(-1, kw))
    dw_ref[...] = dw
    for copy in sends:
        copy.wait_send()
    for condition, make in maybe_sends:
        pl.when(condition)(lambda make=make: make().wait_send())


def settle(*refs):
    count = (len(refs) - 1) // 2
    sems = refs[-1]
    copies = [pltpu.make_async_copy(refs[n], refs[count + n], sems.at[n]) for n in range(count)]
    for copy in copies:
        copy.start()
    for copy in copies:
        copy.wait()


def settled(arrays):
    hbm = pl.BlockSpec(memory_space=pl.ANY)
    vmem = pl.BlockSpec(memory_space=pltpu.VMEM)
    return pl.pallas_call(
        settle,
        out_shape=tuple(jax.ShapeDtypeStruct(a.shape, a.dtype) for a in arrays),
        in_specs=[vmem] * len(arrays),
        out_specs=(hbm,) * len(arrays),
        scratch_shapes=[pltpu.SemaphoreType.DMA((len(arrays),))],
        compiler_params=pltpu.CompilerParams(vmem_limit_bytes=16 * 1024 * 1024),
    )(*arrays)


def fused(sp, tp, scratch, queries, attn_out, log_norm, cotangent, keys, values, source, w_query, w_key, w_value):
    rows = queries.shape[0]
    width = w_value.shape[0]
    vmem, hbm = pl.BlockSpec(memory_space=pltpu.VMEM), pl.BlockSpec(memory_space=pltpu.HBM)
    dma = pltpu.SemaphoreType.DMA
    nz, ny = tp // SIDE, sp // CORES
    return settled(pl.pallas_call(
        functools.partial(kernel, sp, tp),
        out_shape=(
            pltpu.VMEM((rows, width), BF16),
            pltpu.VMEM((source.shape[0], width), BF16),
            pltpu.VMEM(w_value.shape, F32),
        ),
        in_specs=[vmem] * 3 + [hbm] * 7,
        out_specs=(vmem,) * 3,
        scratch_shapes=[pltpu.VMEM(s, t) for s, t in scratch] + [
            dma((3 * HEADS + 9,)), dma((2, sp)), dma((2, sp)), dma((2 * nz,)), dma((tp,)), dma((tp,)), dma((tp,)),
            dma((2 * ny,)), dma((sp,)), dma((sp,)), dma((sp,)), dma((2 * nz,)), dma((tp,)),
            dma((ny, tp)), dma((sp, tp)), dma((sp, tp)), dma((sp, tp)), dma((nz + 1,)), dma((nz + 1,)),
        ],
        compiler_params=pltpu.CompilerParams(
            collective_id=0, has_side_effects=True, vmem_limit_bytes=62 * 1024 * 1024
        ),
    )(log_norm.T, keys, values, queries, attn_out, cotangent, source, w_query, w_key, w_value))


def scratch_of(sp, tp, queries, keys, source, w_query, w_value):
    rows, width = queries.shape
    rs, kw = keys.shape
    stack = (KV_HEADS, rows * HEADS // KV_HEADS, HEAD_DIM)
    flat = stack[:2] + (128,)
    return [
        ((2, tp, sp * rs, kw), BF16), (stack, BF16), (stack, BF16), (stack, BF16),
        (w_query.shape, BF16), (w_value.shape, BF16), (w_value.shape, BF16),
        ((sp,) + source.shape, BF16), ((sp,) + source.shape[::-1], BF16), (flat, F32), (flat, F32), (stack, F32), ((rows, width), BF16),
        ((sp, 2, rs, kw), BF16), ((sp, 2, rs, kw), BF16), ((sp, tp, 2, rs, kw), BF16),
    ]


def shards(sp, tp, *args):
    queries, _, _, _, keys, _, source, w_query, _, w_value = args
    scratch = scratch_of(sp, tp, queries, keys, source, w_query, w_value)
    size = sum(math.prod(s) * jnp.dtype(t).itemsize for s, t in scratch)
    fits = size * 2 < VMEM_BYTES and sp * keys.shape[0] == 128
    if fits and sp % CORES == 0 and tp == 4 * SIDE:
        return fused(sp, tp, scratch, *args)
    return plain(*args)


def plain(queries, attn_out, log_norm, cotangent, keys, values, source, w_query, w_key, w_value):
    single_precision = jnp.float32
    repeat = HEADS // KV_HEADS
    score_scale = 1.0 / math.sqrt(HEAD_DIM)
    rows = queries.shape[0]
    near_keys, near_values = (
        lax.all_gather(keys, "sp", axis=0, tiled=True),
        lax.all_gather(values, "sp", axis=0, tiled=True),
    )
    span = near_keys.shape[0]
    query_tensor4 = queries.reshape(rows, KV_HEADS, repeat, HEAD_DIM)
    output_gradient4 = cotangent.reshape(rows, KV_HEADS, repeat, HEAD_DIM)
    out4 = attn_out.reshape(rows, KV_HEADS, repeat, HEAD_DIM)
    shared_key_heads = near_keys.reshape(span, KV_HEADS, HEAD_DIM)
    shared_value_heads = near_values.reshape(span, KV_HEADS, HEAD_DIM)
    delta = jnp.sum(
        output_gradient4.astype(single_precision) * out4.astype(single_precision), axis=3
    )
    delta = jnp.transpose(delta, (1, 2, 0))[..., None]
    lse = jnp.transpose(log_norm.reshape(rows, KV_HEADS, repeat), (1, 2, 0))[..., None]
    logit_scores = (
        jnp.einsum(
            "znjk,wnk->njzw",
            query_tensor4,
            shared_key_heads,
            preferred_element_type=single_precision,
        )
        * score_scale
    )
    probs = jnp.exp(logit_scores - lse)
    probabilities16 = probs.astype(jnp.bfloat16)
    prob_gradient = jnp.einsum(
        "znjk,wnk->njzw",
        output_gradient4,
        shared_value_heads,
        preferred_element_type=single_precision,
    )
    score_gradient = (probs * (prob_gradient - delta)).astype(jnp.bfloat16)
    query_gradient_piece = (
        jnp.einsum(
            "wohn,nwb->hwob",
            score_gradient,
            shared_key_heads,
            preferred_element_type=single_precision,
        )
        * score_scale
    )
    query_gradient_piece = query_gradient_piece.reshape(rows, -1)
    key_gradient_piece = (
        jnp.einsum(
            "nkjv,jnka->vna", score_gradient, query_tensor4, preferred_element_type=single_precision
        )
        * score_scale
    )
    value_gradient_piece = jnp.einsum(
        "nkjv,jnka->vna", probabilities16, output_gradient4, preferred_element_type=single_precision
    )
    own_keys, own_values = (
        lax.psum_scatter(
            key_gradient_piece.reshape(span, -1).astype(jnp.bfloat16),
            "sp",
            scatter_dimension=0,
            tiled=True,
        ).astype(jnp.float32),
        lax.psum_scatter(
            value_gradient_piece.reshape(span, -1).astype(jnp.bfloat16),
            "sp",
            scatter_dimension=0,
            tiled=True,
        ).astype(jnp.float32),
    )
    stacked = jnp.concatenate(
        [own_keys.astype(jnp.bfloat16), own_values.astype(jnp.bfloat16)], axis=1
    )
    group = lax.all_gather(stacked, "tp", axis=0, tiled=True)
    weights = jnp.concatenate([w_key, w_value], axis=1)
    d_source = lax.dot_general(
        group, weights, (((1,), (1,)), ((), ())), preferred_element_type=single_precision
    ).astype(jnp.bfloat16)
    kv_width = w_value.shape[1]
    weight_term = lax.dot_general(
        source,
        group[:, kv_width:],
        (((0,), (0,)), ((), ())),
        preferred_element_type=single_precision,
    )
    d_wvalue = lax.psum(weight_term.astype(jnp.bfloat16), "sp").astype(jnp.float32)
    dq16 = lax.psum(query_gradient_piece, "tp").astype(jnp.bfloat16)
    d_target = lax.dot_general(
        dq16, w_query, (((1,), (1,)), ((), ())), preferred_element_type=single_precision
    ).astype(jnp.bfloat16)
    return (d_target, d_source, d_wvalue)


def solution(mesh):
    body = functools.partial(shards, mesh.shape["sp"], mesh.shape["tp"])
    in_specs = (
        P("sp", None),
        P("sp", None),
        P("sp", None),
        P("sp", None),
        P(("sp", "tp"), None),
        P(("sp", "tp"), None),
        P("sp", "tp"),
        P("tp", None),
        P("tp", None),
        P("tp", None),
    )
    out_specs = (P("sp", "tp"), P("sp", "tp"), P("tp", None))
    return jax.shard_map(body, mesh=mesh, in_specs=in_specs, out_specs=out_specs, check_vma=False)
```

```python
import functools
import math

import jax
import jax.numpy as jnp
from jax import lax
from jax.experimental import pallas as pl
from jax.experimental.pallas import tpu as pltpu
from jax.sharding import PartitionSpec as P

HEADS = 12
KV_HEADS = 2
HEAD_DIM = 256
CORES = 2
SIDE = 2
VMEM_BYTES = 62 * 1024 * 1024
UNIT = (16, 256)
MESH = pl.DeviceIdType.MESH
NT = (((1,), (1,)), ((), ()))
TN = (((0,), (0,)), ((), ()))
F32 = jnp.float32
BF16 = jnp.bfloat16


def dot(a, b, dims=(((1,), (0,)), ((), ()))):
    return lax.dot_general(a, b, dims, preferred_element_type=F32)


def kernel(
    sp, tp, lse_hbm, k_hbm, v_hbm, q_hbm, o_hbm, do_hbm, src_hbm, wq_hbm, wk_hbm, wv_hbm,
    dt_ref, ds_ref, dw_ref,
    kv, kvs, att, attr, wq, wk, wv, src, src_t, lsev, lse, delta, dqa, dq16, dqs, acc, part, got, full, units,
    load_sem, send_sem, kv_recv, g_recv, gy_recv, one_recv,
):
    rows = q_hbm.shape[0]
    rs, kw = k_hbm.shape
    repeat = HEADS // KV_HEADS
    scale = 1.0 / math.sqrt(HEAD_DIM)
    log2e = math.log2(math.e)
    unit = UNIT[0] * UNIT[1] * 2
    i, j = lax.axis_index("sp"), lax.axis_index("tp")
    nz = tp // SIDE
    y, c = i // CORES, lax.rem(i, CORES)
    z, x = j // SIDE, lax.rem(j, SIDE)
    oy, oc, ox = 1 - y, 1 - c, 1 - x
    orders = [sorted((b for b in range(nz) if b != a), key=lambda b, a=a: abs(a - b)) for a in range(nz)]
    zs = [sum(jnp.where(z == a, order[n], 0) for a, order in enumerate(orders)) for n in range(nz - 1)]
    mid = (z == 1) | (z == 2)
    edge = jnp.where(z == 1, 0, 3)
    jx = z * SIDE + ox
    mine = [a * SIDE + x for a in zs]
    far = [a * SIDE + ox for a in zs]
    at_pair = (y * CORES + oc, j)
    at_y = (oy * CORES + c, j)
    at_x = (i, jx)
    sent = [0, 0]

    def bytes_of(ref):
        return math.prod(ref.shape) * jnp.dtype(ref.dtype).itemsize

    def send(a, b, r, device, s=0):
        pltpu.make_async_remote_copy(
            src_ref=a, dst_ref=b, send_sem=send_sem.at[s], recv_sem=r, device_id=device, device_id_type=MESH,
        ).start()
        if s < 2:
            sent[s] += bytes_of(a)

    def receive(ref, r):
        pltpu.make_async_remote_copy(
            src_ref=ref, dst_ref=ref, send_sem=send_sem.at[0], recv_sem=r, device_id=at_pair, device_id_type=MESH,
        ).wait_recv()

    def load(a, b, s):
        pltpu.make_async_copy(a, b, load_sem.at[s]).start()
        return bytes_of(b)

    def take(size, s):
        ref = units.at[pl.ds(0, size // unit)]
        pltpu.make_async_copy(ref, ref, load_sem.at[s]).wait()

    own = pl.ds(pl.multiple_of(i * rs, rs), rs)
    theirs = pl.ds(pl.multiple_of((y * CORES + oc) * rs, rs), rs)
    kv_size = 0
    for t, r in enumerate((k_hbm, v_hbm)):
        for g in range(KV_HEADS):
            kv_size += load(r.at[:, pl.ds(g * HEAD_DIM, HEAD_DIM)], kvs.at[t, g], 0)
        kv_size += load(r.at[:, pl.ds(pl.multiple_of(c * HEAD_DIM, HEAD_DIM), HEAD_DIM)], kv.at[t, j, own], 0)
    barrier = pltpu.get_barrier_semaphore()

    def signal(device):
        pl.semaphore_signal(barrier, inc=1, device_id=device, device_id_type=MESH)

    near = [at_pair]
    for g in range(CORES):
        near += [(oy * CORES + g, j), (y * CORES + g, jx), (y * CORES + g, mine[0]), (y * CORES + g, mine[1])]
    for d in near:
        signal(d)

    @pl.when(mid)
    def _():
        for g in range(CORES):
            signal((y * CORES + g, mine[2]))

    def load_heads(g, a, r, s):
        size = 0
        for h in range(repeat):
            columns = pl.ds(pl.multiple_of((g * repeat + h) * HEAD_DIM, HEAD_DIM), HEAD_DIM)
            size += load(r.at[:, columns], att.at[a, g, pl.ds(h * rows, rows)], s)
        return size

    attn = (q_hbm, do_hbm, o_hbm)
    head_size = [load_heads(oc, a, r, 1 + a) for a, r in enumerate(attn)][0]
    own_size = sum(load_heads(c, a, r, 4) for a, r in enumerate(attn))
    load(lse_hbm, lsev.at[0], 5)
    src_size = load(src_hbm, src.at[c, y], 6)
    weight_size = load(wk_hbm, wk, 7) + load(wv_hbm, wv, 7)
    half = wq.shape[2]
    for g in range(KV_HEADS):
        weight_size += load(wq_hbm.at[:, pl.ds(g * half, half)], wq.at[g], 7)
    take(kv_size, 0)
    pl.semaphore_wait(barrier, len(near) + 2 * mid.astype(jnp.int32))


    def raw(y_to, slot, s=0):
        for g in range(CORES):
            send(kvs.at[:, g], kv.at[:, j, own], kv_recv.at[j, y], (y_to * CORES + g, slot), s)

    raw(oy, j)
    raw(y, jx)
    raw(y, mine[0])
    raw(y, mine[1])

    @pl.when(mid)
    def _():
        raw(y, mine[2], 1)

    send(kvs.at[:, oc], kv.at[:, j, own], kv_recv.at[j, y], at_pair)
    for a in range(3):
        take(head_size, 1 + a)
        send(att.at[a, oc], attr.at[a], one_recv.at[0], at_pair)
    pltpu.make_async_copy(lse_hbm, lsev.at[0], load_sem.at[5]).wait()
    send(lsev.at[0], lsev.at[1], one_recv.at[1], at_pair, 2)
    take(own_size, 4)

    def block(b, a):
        return att[a, c] if b == 0 else attr[a]

    def statistics(b):
        for h in range(repeat):
            at = pl.ds(h * rows, rows)
            do, o = (att[a, c, at] if b == 0 else attr[a, at] for a in (1, 2))
            d = jnp.sum(do.astype(F32) * o.astype(F32), axis=1, keepdims=True)
            delta[b, at] = jnp.broadcast_to(d, (rows, 128))
            row = jnp.where(c == 0, lsev[b, h:h + 1, :], lsev[b, repeat + h:repeat + h + 1, :])
            lse[b, at] = jnp.transpose(jnp.broadcast_to(row * log2e, (128, rows)))

    statistics(0)

    def piece(slot, h):
        return kv.at[:, slot, pl.ds(pl.multiple_of(h * (CORES * rs), CORES * rs), CORES * rs)]

    def arrived(slot, h):
        receive(piece(slot, h), kv_recv.at[slot, h])

    def relay(slot, h, device, s=0):
        send(piece(slot, h), piece(slot, h), kv_recv.at[slot, h], device, s)

    def from_z(n, h):
        arrived(mine[n], h)
        relay(mine[n], h, at_x)
        if n == nz - 2:
            pl.when(mid)(lambda: relay(mine[n], h, (i, edge * SIDE + x), 1))

    receive(kv.at[:, j, theirs], kv_recv.at[j, y])
    arrived(j, oy)
    relay(j, oy, at_x)
    relay(j, oy, (i, mine[0]))
    relay(j, oy, (i, mine[1]))
    pl.when(mid)(lambda: relay(j, oy, (i, mine[2]), 1))
    from_z(0, y)
    receive(attr, one_recv.at[0])
    receive(lsev.at[1], one_recv.at[1])
    statistics(1)

    def wide(a, n):
        return a if n == 1 else jnp.concatenate([a] * n, axis=1)

    def grads(b, keys, values):
        n = keys.shape[0] // 128
        p = jnp.exp2(dot(block(b, 0), keys, NT) * (scale * log2e) - wide(lse[b], n))
        dp = dot(block(b, 1), values, NT)
        return p, (p * (dp - wide(delta[b], n))).astype(BF16)

    def local(b):
        keys = kv[0, j]
        p, ds = grads(b, keys, kv[1, j])
        dk = dot(ds, block(b, 0), TN)
        dv = dot(p.astype(BF16), block(b, 1), TN)
        dqa[b] = dot(ds, keys)
        if b == 0:
            acc[0] = dk
            acc[1] = dv
        else:
            part[:, 0] = ((acc[0] + dk) * scale).astype(BF16).reshape(sp, rs, HEAD_DIM)
            part[:, 1] = (acc[1] + dv).astype(BF16).reshape(sp, rs, HEAD_DIM)

    local(0)
    from_z(1, y)
    local(1)
    for g in range(CORES):
        to = oy * CORES + g
        send(part.at[to], got.at[1 + c], one_recv.at[2], (to, j))
    send(part.at[y * CORES + oc], got.at[0], one_recv.at[2], at_pair)
    take(src_size, 6)
    for device, r in ((at_y, 3), (at_pair, 4)):
        send(src.at[c, y], src.at[c, y], one_recv.at[r], device)

    def chunk(slots, order=(0, 1)):
        for b in order:
            keys, values = (kv[t, slots].reshape(-1, HEAD_DIM) for t in range(2))
            _, ds = grads(b, keys, values)
            dqa[b] += dot(ds, keys)

    arrived(jx, y)
    arrived(jx, oy)
    chunk(pl.ds(jx, 1))
    from_z(0, oy)
    from_z(1, oy)
    receive(got, one_recv.at[2])
    here = part[i].astype(F32) + got[1 + c].astype(F32)
    there = got[0].astype(F32) + got[1 + oc].astype(F32)
    for g in range(KV_HEADS):
        full[c, y, j, :, :, g * HEAD_DIM:(g + 1) * HEAD_DIM] = jnp.where(c == g, here, there).astype(BF16)

    def g_send(slot, device, only=None, s=0):
        ref = full.at[c, y, slot] if only is None else full.at[c, y, slot, only]
        send(ref, ref, g_recv.at[slot, only or 0], device, s)

    def g_arrived(slot, only=None):
        receive(full.at[c, y, slot] if only is None else full.at[c, y, slot, only], g_recv.at[slot, only or 0])

    def g_spread(slot):
        ref = full.at[c, y, slot, 1]
        send(ref, ref, gy_recv.at[slot], at_y)
        send(ref, ref, one_recv.at[5], at_pair)

    def g_from_y(slot):
        ref = full.at[c, oy, slot, 1]
        receive(ref, gy_recv.at[slot])
        send(ref, ref, one_recv.at[5], at_pair)

    def g_from_x():
        g_arrived(jx)
        g_send(jx, (i, mine[0]), 1)
        g_send(jx, (i, mine[1]), 1)
        pl.when(mid)(lambda: g_send(jx, (i, mine[2]), 1, 1))
        g_spread(jx)

    def g_from_z(n):
        g_arrived(mine[n])
        if n == nz - 2:
            pl.when(mid)(lambda: g_send(mine[n], (i, edge * SIDE + x), None, 1))
        g_send(mine[n], at_x, 0)
        g_spread(mine[n])

    def g_from_far(n):
        g_arrived(far[n], 1)
        if n == nz - 2:
            pl.when(mid)(lambda: g_send(far[n], (i, edge * SIDE + x), 1, 1))
        g_spread(far[n])

    g_send(j, at_x)
    g_send(j, (i, mine[0]))
    g_send(j, (i, mine[1]))
    pl.when(mid)(lambda: g_send(j, (i, mine[2]), None, 1))
    g_spread(j)
    from_z(2, y)
    from_z(2, oy)

    def chunk_z(n, order=(0, 1)):
        chunk(pl.ds(zs[n] * SIDE, SIDE), order)

    def far_arrived(n):
        arrived(far[n], y)
        arrived(far[n], oy)

    far_arrived(0)
    chunk_z(0)
    g_from_x()
    g_from_z(0)
    far_arrived(1)
    chunk_z(1)
    g_from_z(1)
    g_from_far(0)
    receive(src.at[c, oy], one_recv.at[3])
    send(src.at[c, oy], src.at[c, oy], one_recv.at[4], at_pair)
    g_from_y(j)
    g_from_z(2)
    far_arrived(2)
    chunk_z(2, (1,))

    def rounded(b, ref):
        for h in range(repeat):
            ref[:, h * HEAD_DIM:(h + 1) * HEAD_DIM] = (dqa[b, h * rows:(h + 1) * rows] * scale).astype(BF16)

    rounded(1, dqs)
    send(dqs, dq16.at[c], one_recv.at[6], at_pair)
    g_from_far(1)
    chunk_z(2, (0,))
    rounded(0, dq16.at[c])
    g_from_far(2)
    for slot in [jx, mine[0], mine[1], far[0]]:
        g_from_y(slot)
    take(weight_size, 7)
    receive(src.at[oc], one_recv.at[4])
    for a in range(CORES):
        for b in range(sp // CORES):
            src_t[a, b] = jnp.transpose(src[a, b])
    receive(dq16.at[oc], one_recv.at[6])
    dt_ref[...] = (dot(dq16[0], wq[0], NT) + dot(dq16[1], wq[1], NT)).astype(BF16)
    g_from_y(mine[2])
    g_from_y(far[1])
    for n in range(nz - 1):
        g_arrived(far[n], 0)
    ds_ref[...] = (
        dot(full[c, y, :, 0].reshape(-1, kw), wk[...], NT) + dot(full[c, y, :, 1].reshape(-1, kw), wv[...], NT)
    ).astype(BF16)
    g_from_y(far[2])
    receive(full.at[oc, :, :, 1], one_recv.at[5])
    dw = None
    for b in range(sp // CORES):
        for a in range(CORES):
            term = dot(src_t[a, b], full[a, b, :, 1].reshape(-1, kw))
            dw = term if dw is None else dw + term
    dw_ref[...] = dw

    def sent_all(s):
        ref = units.at[pl.ds(0, sent[s] // unit)]
        pltpu.make_async_remote_copy(
            src_ref=ref, dst_ref=ref, send_sem=send_sem.at[s], recv_sem=one_recv.at[0],
            device_id=at_pair, device_id_type=MESH,
        ).wait_send()

    sent_all(0)
    pl.when(mid)(lambda: sent_all(1))
    pltpu.make_async_remote_copy(
        src_ref=lsev.at[0], dst_ref=lsev.at[1], send_sem=send_sem.at[2], recv_sem=one_recv.at[1],
        device_id=at_pair, device_id_type=MESH,
    ).wait_send()


def settle(*refs):
    count = (len(refs) - 1) // 2
    sems = refs[-1]
    copies = [pltpu.make_async_copy(refs[n], refs[count + n], sems.at[n]) for n in range(count)]
    for copy in copies:
        copy.start()
    for copy in copies:
        copy.wait()


def settled(arrays):
    hbm = pl.BlockSpec(memory_space=pl.ANY)
    vmem = pl.BlockSpec(memory_space=pltpu.VMEM)
    return pl.pallas_call(
        settle,
        out_shape=tuple(jax.ShapeDtypeStruct(a.shape, a.dtype) for a in arrays),
        in_specs=[vmem] * len(arrays),
        out_specs=(hbm,) * len(arrays),
        scratch_shapes=[pltpu.SemaphoreType.DMA((len(arrays),))],
        compiler_params=pltpu.CompilerParams(vmem_limit_bytes=16 * 1024 * 1024),
    )(*arrays)


def fused(sp, tp, queries, attn_out, log_norm, cotangent, keys, values, source, w_query, w_key, w_value):
    rows, model = queries.shape
    width = w_value.shape[0]
    rs, kw = keys.shape
    vmem, hbm = pl.BlockSpec(memory_space=pltpu.VMEM), pl.BlockSpec(memory_space=pl.ANY)
    dma = pltpu.SemaphoreType.DMA
    stack = (rows * HEADS // KV_HEADS, HEAD_DIM)
    half = model // KV_HEADS
    ny = sp // CORES
    scratch = [
        ((2, tp, sp * rs, HEAD_DIM), BF16), ((2, KV_HEADS, rs, HEAD_DIM), BF16),
        ((3, KV_HEADS) + stack, BF16), ((3,) + stack, BF16),
        ((KV_HEADS, width, half), BF16), (w_key.shape, BF16), (w_value.shape, BF16),
        ((CORES, ny) + source.shape, BF16), ((CORES, ny) + source.shape[::-1], BF16),
        ((2, HEADS, rows), F32), ((2, stack[0], 128), F32), ((2, stack[0], 128), F32),
        ((2,) + stack, F32), ((KV_HEADS, rows, half), BF16), ((rows, half), BF16),
        ((2, sp * rs, HEAD_DIM), F32), ((sp, 2, rs, HEAD_DIM), BF16), ((3, 2, rs, HEAD_DIM), BF16),
        ((CORES, ny, tp, 2, rs, kw), BF16), ((640,) + UNIT, BF16),
    ]
    return settled(pl.pallas_call(
        functools.partial(kernel, sp, tp),
        out_shape=(
            pltpu.VMEM((rows, width), BF16),
            pltpu.VMEM((source.shape[0], width), BF16),
            pltpu.VMEM(w_value.shape, F32),
        ),
        in_specs=[hbm] * 10,
        out_specs=(vmem,) * 3,
        scratch_shapes=[pltpu.VMEM(s, t) for s, t in scratch] + [
            dma((8,)), dma((3,)), dma((tp, ny)), dma((tp, 2)), dma((tp,)), dma((7,)),
        ],
        compiler_params=pltpu.CompilerParams(
            collective_id=0, has_side_effects=True, vmem_limit_bytes=VMEM_BYTES
        ),
    )(log_norm.T, keys, values, queries, attn_out, cotangent, source, w_query, w_key, w_value))


def shards(sp, tp, *args):
    queries, keys, source = args[0], args[4], args[6]
    if sp == 2 * CORES and tp == 4 * SIDE and queries.shape[0] == 128 and sp * keys.shape[0] == 128 and source.shape[0] == 256:
        return fused(sp, tp, *args)
    return plain(*args)


def plain(queries, attn_out, log_norm, cotangent, keys, values, source, w_query, w_key, w_value):
    single_precision = jnp.float32
    repeat = HEADS // KV_HEADS
    score_scale = 1.0 / math.sqrt(HEAD_DIM)
    rows = queries.shape[0]
    near_keys, near_values = (
        lax.all_gather(keys, "sp", axis=0, tiled=True),
        lax.all_gather(values, "sp", axis=0, tiled=True),
    )
    span = near_keys.shape[0]
    query_tensor4 = queries.reshape(rows, KV_HEADS, repeat, HEAD_DIM)
    output_gradient4 = cotangent.reshape(rows, KV_HEADS, repeat, HEAD_DIM)
    out4 = attn_out.reshape(rows, KV_HEADS, repeat, HEAD_DIM)
    shared_key_heads = near_keys.reshape(span, KV_HEADS, HEAD_DIM)
    shared_value_heads = near_values.reshape(span, KV_HEADS, HEAD_DIM)
    delta = jnp.sum(
        output_gradient4.astype(single_precision) * out4.astype(single_precision), axis=3
    )
    delta = jnp.transpose(delta, (1, 2, 0))[..., None]
    lse = jnp.transpose(log_norm.reshape(rows, KV_HEADS, repeat), (1, 2, 0))[..., None]
    logit_scores = (
        jnp.einsum(
            "znjk,wnk->njzw",
            query_tensor4,
            shared_key_heads,
            preferred_element_type=single_precision,
        )
        * score_scale
    )
    probs = jnp.exp(logit_scores - lse)
    probabilities16 = probs.astype(jnp.bfloat16)
    prob_gradient = jnp.einsum(
        "znjk,wnk->njzw",
        output_gradient4,
        shared_value_heads,
        preferred_element_type=single_precision,
    )
    score_gradient = (probs * (prob_gradient - delta)).astype(jnp.bfloat16)
    query_gradient_piece = (
        jnp.einsum(
            "wohn,nwb->hwob",
            score_gradient,
            shared_key_heads,
            preferred_element_type=single_precision,
        )
        * score_scale
    )
    query_gradient_piece = query_gradient_piece.reshape(rows, -1)
    key_gradient_piece = (
        jnp.einsum(
            "nkjv,jnka->vna", score_gradient, query_tensor4, preferred_element_type=single_precision
        )
        * score_scale
    )
    value_gradient_piece = jnp.einsum(
        "nkjv,jnka->vna", probabilities16, output_gradient4, preferred_element_type=single_precision
    )
    own_keys, own_values = (
        lax.psum_scatter(
            key_gradient_piece.reshape(span, -1).astype(jnp.bfloat16),
            "sp",
            scatter_dimension=0,
            tiled=True,
        ).astype(jnp.float32),
        lax.psum_scatter(
            value_gradient_piece.reshape(span, -1).astype(jnp.bfloat16),
            "sp",
            scatter_dimension=0,
            tiled=True,
        ).astype(jnp.float32),
    )
    stacked = jnp.concatenate(
        [own_keys.astype(jnp.bfloat16), own_values.astype(jnp.bfloat16)], axis=1
    )
    group = lax.all_gather(stacked, "tp", axis=0, tiled=True)
    weights = jnp.concatenate([w_key, w_value], axis=1)
    d_source = lax.dot_general(
        group, weights, (((1,), (1,)), ((), ())), preferred_element_type=single_precision
    ).astype(jnp.bfloat16)
    kv_width = w_value.shape[1]
    weight_term = lax.dot_general(
        source,
        group[:, kv_width:],
        (((0,), (0,)), ((), ())),
        preferred_element_type=single_precision,
    )
    d_wvalue = lax.psum(weight_term.astype(jnp.bfloat16), "sp").astype(jnp.float32)
    dq16 = lax.psum(query_gradient_piece, "tp").astype(jnp.bfloat16)
    d_target = lax.dot_general(
        dq16, w_query, (((1,), (1,)), ((), ())), preferred_element_type=single_precision
    ).astype(jnp.bfloat16)
    return (d_target, d_source, d_wvalue)


def solution(mesh):
    body = functools.partial(shards, mesh.shape["sp"], mesh.shape["tp"])
    in_specs = (
        P("sp", None),
        P("sp", None),
        P("sp", None),
        P("sp", None),
        P(("sp", "tp"), None),
        P(("sp", "tp"), None),
        P("sp", "tp"),
        P("tp", None),
        P("tp", None),
        P("tp", None),
    )
    out_specs = (P("sp", "tp"), P("sp", "tp"), P("tp", None))
    return jax.shard_map(body, mesh=mesh, in_specs=in_specs, out_specs=out_specs, check_vma=False)
```

```python
import functools
import math

import jax
import jax.numpy as jnp
from jax import lax
from jax.experimental import pallas as pl
from jax.experimental.pallas import tpu as pltpu
from jax.sharding import PartitionSpec as P

HEADS = 12
KV_HEADS = 2
HEAD_DIM = 256
CORES = 2
SIDE = 2
VMEM_BYTES = 62 * 1024 * 1024
UNIT = (16, 256)
MESH = pl.DeviceIdType.MESH
NT = (((1,), (1,)), ((), ()))
TN = (((0,), (0,)), ((), ()))
F32 = jnp.float32
BF16 = jnp.bfloat16


def dot(a, b, dims=(((1,), (0,)), ((), ()))):
    return lax.dot_general(a, b, dims, preferred_element_type=F32)


def kernel(
    sp, tp, lse_hbm, k_hbm, v_hbm, q_hbm, o_hbm, do_hbm, src_hbm, wq_hbm, wk_hbm, wv_hbm,
    dt_ref, ds_ref, dw_ref,
    kv, kvs, att, attr, wq, wk, wv, wqt, wkt, wvt, src, src_t, lsev, lse, delta, dqa, dq16, dqs, acc, prob,
    part, got, dkf, dvf, units,
    load_sem, send_sem, kv_recv, g_recv, gy_recv, one_recv,
):
    rows = q_hbm.shape[0]
    rs, kw = k_hbm.shape
    repeat = HEADS // KV_HEADS
    scale = 1.0 / math.sqrt(HEAD_DIM)
    log2e = math.log2(math.e)
    unit = UNIT[0] * UNIT[1] * 2
    i, j = lax.axis_index("sp"), lax.axis_index("tp")
    nz = tp // SIDE
    y, c = i // CORES, lax.rem(i, CORES)
    z, x = j // SIDE, lax.rem(j, SIDE)
    oy, oc, ox = 1 - y, 1 - c, 1 - x
    orders = [sorted((b for b in range(nz) if b != a), key=lambda b, a=a: abs(a - b)) for a in range(nz)]
    zs = [sum(jnp.where(z == a, order[n], 0) for a, order in enumerate(orders)) for n in range(nz - 1)]
    mid = (z == 1) | (z == 2)
    edge = jnp.where(z == 1, 0, 3)
    jx = z * SIDE + ox
    mine = [a * SIDE + x for a in zs]
    far = [a * SIDE + ox for a in zs]
    at_pair = (y * CORES + oc, j)
    at_y = (oy * CORES + c, j)
    at_x = (i, jx)
    sent = [0, 0]

    def bytes_of(ref):
        return math.prod(ref.shape) * jnp.dtype(ref.dtype).itemsize

    def send(a, b, r, device, s=0):
        pltpu.make_async_remote_copy(
            src_ref=a, dst_ref=b, send_sem=send_sem.at[s % 3], recv_sem=r, device_id=device, device_id_type=MESH,
        ).start()
        if s < 2:
            sent[s] += bytes_of(a)

    def receive(ref, r):
        pltpu.make_async_remote_copy(
            src_ref=ref, dst_ref=ref, send_sem=send_sem.at[0], recv_sem=r, device_id=at_pair, device_id_type=MESH,
        ).wait_recv()

    def load(a, b, s):
        pltpu.make_async_copy(a, b, load_sem.at[s]).start()
        return bytes_of(b)

    def take(size, s):
        ref = units.at[pl.ds(0, size // unit)]
        pltpu.make_async_copy(ref, ref, load_sem.at[s]).wait()

    own = pl.ds(pl.multiple_of(i * rs, rs), rs)
    theirs = pl.ds(pl.multiple_of((y * CORES + oc) * rs, rs), rs)
    kv_size = 0
    for t, r in enumerate((k_hbm, v_hbm)):
        for g in range(KV_HEADS):
            kv_size += load(r.at[:, pl.ds(g * HEAD_DIM, HEAD_DIM)], kvs.at[t, g], 0)
        kv_size += load(r.at[:, pl.ds(pl.multiple_of(c * HEAD_DIM, HEAD_DIM), HEAD_DIM)], kv.at[t, j, own], 0)
    barrier = pltpu.get_barrier_semaphore()

    def signal(device):
        pl.semaphore_signal(barrier, inc=1, device_id=device, device_id_type=MESH)

    near = [at_pair]
    for g in range(CORES):
        near += [(oy * CORES + g, j), (y * CORES + g, jx), (y * CORES + g, mine[0]), (y * CORES + g, mine[1])]
    for d in near:
        signal(d)

    @pl.when(mid)
    def _():
        for g in range(CORES):
            signal((y * CORES + g, mine[2]))

    def load_heads(g, a, r, s):
        size = 0
        for h in range(repeat):
            columns = pl.ds(pl.multiple_of((g * repeat + h) * HEAD_DIM, HEAD_DIM), HEAD_DIM)
            size += load(r.at[:, columns], att.at[a, g, pl.ds(h * rows, rows)], s)
        return size

    attn = (q_hbm, do_hbm, o_hbm)
    head_size = [load_heads(oc, a, r, 1 + a) for a, r in enumerate(attn)][0]
    own_size = sum(load_heads(c, a, r, 4) for a, r in enumerate(attn))
    load(lse_hbm, lsev.at[0], 5)
    src_size = load(src_hbm, src.at[c, y], 6)
    weight_size = load(wk_hbm, wk, 7) + load(wv_hbm, wv, 7)
    weight_size += load(wq_hbm, wq, 7)
    take(kv_size, 0)
    pl.semaphore_wait(barrier, len(near) + 2 * mid.astype(jnp.int32))


    def raw(y_to, slot, s=0):
        for g in range(CORES):
            send(kvs.at[:, g], kv.at[:, j, own], kv_recv.at[j, y], (y_to * CORES + g, slot), s)

    raw(oy, j)
    raw(y, jx)
    raw(y, mine[0])
    raw(y, mine[1])

    @pl.when(mid)
    def _():
        raw(y, mine[2], 1)

    send(kvs.at[:, oc], kv.at[:, j, own], kv_recv.at[j, y], at_pair)
    for a in range(3):
        take(head_size, 1 + a)
        send(att.at[a, oc], attr.at[a], one_recv.at[0 if a < 2 else 7], at_pair)
    pltpu.make_async_copy(lse_hbm, lsev.at[0], load_sem.at[5]).wait()
    send(lsev.at[0], lsev.at[1], one_recv.at[1], at_pair, 2)
    take(own_size, 4)

    def block(b, a):
        return att[a, c] if b == 0 else attr[a]

    def deltas(b):
        for h in range(repeat):
            at = pl.ds(h * rows, rows)
            do, o = (att[a, c, at] if b == 0 else attr[a, at] for a in (1, 2))
            d = jnp.sum(do.astype(F32) * o.astype(F32), axis=1, keepdims=True)
            delta[b, at] = jnp.broadcast_to(d, (rows, 128))

    def norms(b):
        for h in range(repeat):
            row = jnp.where(c == 0, lsev[b, h:h + 1, :], lsev[b, repeat + h:repeat + h + 1, :])
            lse[b, pl.ds(h * rows, rows)] = jnp.transpose(jnp.broadcast_to(row * log2e, (128, rows)))

    norms(0)
    deltas(0)
    take(weight_size, 7)
    for n in range(repeat):
        columns = slice(n * kw, (n + 1) * kw)
        wqt[columns, :] = jnp.transpose(wq[:, columns])
    wkt[...] = jnp.transpose(wk[...])
    wvt[...] = jnp.transpose(wv[...])

    def piece(slot, h):
        return kv.at[:, slot, pl.ds(pl.multiple_of(h * (CORES * rs), CORES * rs), CORES * rs)]

    def arrived(slot, h):
        receive(piece(slot, h), kv_recv.at[slot, h])

    def relay(slot, h, device, s=0):
        send(piece(slot, h), piece(slot, h), kv_recv.at[slot, h], device, s)

    def from_z(n, h):
        arrived(mine[n], h)
        relay(mine[n], h, at_x)

    def last_z(h, early):
        def body():
            arrived(mine[nz - 2], h)
            if early:
                relay(mine[nz - 2], h, (i, edge * SIDE + x), 1)
            relay(mine[nz - 2], h, at_x, 0 if early else 3)

        pl.when(mid if early else jnp.logical_not(mid))(body)

    receive(kv.at[:, j, theirs], kv_recv.at[j, y])
    arrived(j, oy)
    relay(j, oy, (i, mine[0]))
    relay(j, oy, (i, mine[1]))
    pl.when(mid)(lambda: relay(j, oy, (i, mine[2]), 1))
    from_z(0, y)
    receive(attr.at[pl.ds(0, 2)], one_recv.at[0])
    receive(lsev.at[1], one_recv.at[1])
    norms(1)

    def wide(a, n):
        return a if n == 1 else jnp.concatenate([a] * n, axis=1)

    def probs(b, keys):
        return jnp.exp2(dot(block(b, 0), keys, NT) * (scale * log2e) - wide(lse[b], keys.shape[0] // 128))

    def scores(b, p, values):
        dp = dot(block(b, 1), values, NT)
        return (p * (dp - wide(delta[b], values.shape[0] // 128))).astype(BF16)

    def part_send(t, r):
        for g in range(CORES):
            to = oy * CORES + g
            send(part.at[t, to], got.at[t, 1 + c], r, (to, j))
        send(part.at[t, y * CORES + oc], got.at[t, 0], r, at_pair)

    for b in range(2):
        p = probs(b, kv[0, j])
        prob[b] = p
        dv = dot(p.astype(BF16), block(b, 1), TN)
        if b == 0:
            acc[1] = dv
        else:
            part[1] = (acc[1] + dv).astype(BF16).reshape(sp, rs, HEAD_DIM)
    part_send(1, one_recv.at[2])
    arrived(jx, y)
    relay(jx, y, at_y)
    last_z(y, True)
    receive(attr.at[2], one_recv.at[7])
    deltas(1)
    for b in range(2):
        keys = kv[0, j]
        ds = scores(b, prob[b], kv[1, j])
        dk = dot(ds, block(b, 0), TN)
        dqa[b] = dot(ds, keys)
        if b == 0:
            acc[0] = dk
        else:
            part[0] = ((acc[0] + dk) * scale).astype(BF16).reshape(sp, rs, HEAD_DIM)
    part_send(0, one_recv.at[8])
    take(src_size, 6)
    for device, r in ((at_y, 3), (at_pair, 4)):
        send(src.at[c, y], src.at[c, y], one_recv.at[r], device)

    def chunk(slots, order=(0, 1)):
        for b in order:
            keys, values = (kv[t, slots].reshape(-1, HEAD_DIM) for t in range(2))
            dqa[b] += dot(scores(b, probs(b, keys), values), keys)

    def total(t):
        here = part[t, i].astype(F32) + got[t, 1 + c].astype(F32)
        there = got[t, 0].astype(F32) + got[t, 1 + oc].astype(F32)
        ref = dkf.at[j] if t == 0 else dvf.at[c, y, j]
        for g in range(KV_HEADS):
            ref[:, g * HEAD_DIM:(g + 1) * HEAD_DIM] = jnp.where(c == g, here, there).astype(BF16)

    def grad(t, slot):
        return dkf.at[slot] if t == 0 else dvf.at[c, y, slot]

    def g_send(t, slot, device, s=0):
        send(grad(t, slot), grad(t, slot), g_recv.at[slot, t], device, s)

    def g_arrived(t, slot):
        receive(grad(t, slot), g_recv.at[slot, t])

    def g_along_z(t, slot):
        g_send(t, slot, (i, mine[0]))
        g_send(t, slot, (i, mine[1]))
        pl.when(mid)(lambda: g_send(t, slot, (i, mine[2]), 1))

    def g_spread(slot, last=False, s=0):
        ref = grad(1, slot)
        send(ref, ref, gy_recv.at[slot], at_y, s)
        send(ref, ref, one_recv.at[5], at_pair, s)
        if last:
            send(ref, ref, one_recv.at[5], (oy * CORES + oc, j), s)

    def g_from_y(slot, last=False):
        ref = dvf.at[c, oy, slot]
        receive(ref, gy_recv.at[slot])
        if not last:
            send(ref, ref, one_recv.at[5], at_pair)

    def dv_from(slot):
        g_arrived(1, slot)
        g_spread(slot)

    def dv_last(slot, early, last=False):
        def body():
            g_arrived(1, slot)
            if early:
                g_send(1, slot, (i, edge * SIDE + x), 1)
            g_spread(slot, last, 0 if early else 3)

        pl.when(mid if early else jnp.logical_not(mid))(body)

    def dk_from(n):
        g_arrived(0, mine[n])
        g_send(0, mine[n], at_x)

    def dk_last(early):
        def body():
            g_arrived(0, mine[nz - 2])
            if early:
                g_send(0, mine[nz - 2], (i, edge * SIDE + x), 1)
            g_send(0, mine[nz - 2], at_x, 0 if early else 3)

        pl.when(mid if early else jnp.logical_not(mid))(body)

    def chunk_z(n, order=(0, 1)):
        chunk(pl.ds(zs[n] * SIDE, SIDE), order)

    def far_arrived(n):
        arrived(far[n], y)
        arrived(far[n], oy)

    from_z(1, y)
    receive(got.at[1], one_recv.at[2])
    total(1)
    g_send(1, j, at_x)
    g_along_z(1, j)
    g_spread(j)
    from_z(0, oy)
    last_z(oy, True)
    arrived(jx, oy)
    chunk(pl.ds(jx, 1))
    receive(got.at[0], one_recv.at[8])
    total(0)
    g_along_z(0, j)
    g_send(0, j, at_x)
    from_z(1, oy)
    g_arrived(1, jx)
    g_along_z(1, jx)
    g_spread(jx)
    dv_from(mine[0])
    last_z(y, False)
    last_z(oy, False)
    dv_last(mine[2], True)
    far_arrived(0)
    chunk_z(0)
    dv_from(mine[1])
    dv_from(far[0])
    dv_last(far[2], True, True)
    far_arrived(1)
    chunk_z(1)
    dv_last(mine[2], False)
    dv_from(far[1])
    receive(src.at[c, oy], one_recv.at[3])
    send(src.at[c, oy], src.at[c, oy], one_recv.at[4], at_pair)
    dk_from(0)
    dk_from(1)
    g_from_y(j)
    g_from_y(jx)
    dk_last(True)
    far_arrived(2)
    chunk_z(2, (1,))

    def rounded(b, ref):
        for h in range(repeat):
            ref[:, h * HEAD_DIM:(h + 1) * HEAD_DIM] = (dqa[b, h * rows:(h + 1) * rows] * scale).astype(BF16)

    half = dqs.shape[1]
    rounded(1, dqs)
    send(dqs, dq16.at[:, pl.ds(pl.multiple_of(c * half, half), half)], one_recv.at[6], at_pair)
    dv_last(far[2], False, True)
    dk_last(False)
    chunk_z(2, (0,))
    for h in range(repeat):
        at = pl.ds(pl.multiple_of(c * half + h * HEAD_DIM, HEAD_DIM), HEAD_DIM)
        dq16[:, at] = (dqa[0, h * rows:(h + 1) * rows] * scale).astype(BF16)
    for slot in [mine[0], mine[1], far[0], mine[2], far[1]]:
        g_from_y(slot)
    receive(src.at[oc], one_recv.at[4])
    deep = src.shape[2]
    for b in range(sp // CORES):
        for a in range(CORES):
            n = b * CORES + a
            src_t[:, n * deep:(n + 1) * deep] = jnp.transpose(src[a, b])
    receive(dq16.at[:, pl.ds(pl.multiple_of(oc * half, half), half)], one_recv.at[6])
    dt_ref[...] = dot(dq16[...], wqt[...]).astype(BF16)
    g_arrived(0, jx)
    for n in range(nz - 1):
        g_arrived(0, far[n])
    ds_ref[...] = (
        dot(dkf[...].reshape(-1, kw), wkt[...]) + dot(dvf[c, y].reshape(-1, kw), wvt[...])
    ).astype(BF16)
    g_from_y(far[2], True)
    receive(dvf.at[oc], one_recv.at[5])
    dw_ref[...] = dot(src_t[...], jnp.concatenate(
        [dvf[a, b].reshape(-1, kw) for b in range(sp // CORES) for a in range(CORES)], axis=0))

    def sent_all(s):
        ref = units.at[pl.ds(0, sent[s] // unit)]
        pltpu.make_async_remote_copy(
            src_ref=ref, dst_ref=ref, send_sem=send_sem.at[s], recv_sem=one_recv.at[0],
            device_id=at_pair, device_id_type=MESH,
        ).wait_send()

    sent_all(0)
    pl.when(mid)(lambda: sent_all(1))
    pltpu.make_async_remote_copy(
        src_ref=lsev.at[0], dst_ref=lsev.at[1], send_sem=send_sem.at[2], recv_sem=one_recv.at[1],
        device_id=at_pair, device_id_type=MESH,
    ).wait_send()


def settle(*refs):
    count = (len(refs) - 1) // 2
    sems = refs[-1]
    copies = [pltpu.make_async_copy(refs[n], refs[count + n], sems.at[n]) for n in range(count)]
    for copy in copies:
        copy.start()
    for copy in copies:
        copy.wait()


def settled(arrays):
    hbm = pl.BlockSpec(memory_space=pl.ANY)
    vmem = pl.BlockSpec(memory_space=pltpu.VMEM)
    return pl.pallas_call(
        settle,
        out_shape=tuple(jax.ShapeDtypeStruct(a.shape, a.dtype) for a in arrays),
        in_specs=[vmem] * len(arrays),
        out_specs=(hbm,) * len(arrays),
        scratch_shapes=[pltpu.SemaphoreType.DMA((len(arrays),))],
        compiler_params=pltpu.CompilerParams(vmem_limit_bytes=16 * 1024 * 1024),
    )(*arrays)


def fused(sp, tp, queries, attn_out, log_norm, cotangent, keys, values, source, w_query, w_key, w_value):
    rows, model = queries.shape
    width = w_value.shape[0]
    rs, kw = keys.shape
    vmem, hbm = pl.BlockSpec(memory_space=pltpu.VMEM), pl.BlockSpec(memory_space=pl.ANY)
    dma = pltpu.SemaphoreType.DMA
    stack = (rows * HEADS // KV_HEADS, HEAD_DIM)
    half = model // KV_HEADS
    ny = sp // CORES
    scratch = [
        ((2, tp, sp * rs, HEAD_DIM), BF16), ((2, KV_HEADS, rs, HEAD_DIM), BF16),
        ((3, KV_HEADS) + stack, BF16), ((3,) + stack, BF16),
        (w_query.shape, BF16), (w_key.shape, BF16), (w_value.shape, BF16),
        (w_query.shape[::-1], BF16), (w_key.shape[::-1], BF16), (w_value.shape[::-1], BF16),
        ((CORES, ny) + source.shape, BF16), ((width, sp * source.shape[0]), BF16),
        ((2, HEADS, rows), F32), ((2, stack[0], 128), F32), ((2, stack[0], 128), F32),
        ((2,) + stack, F32), ((rows, model), BF16), ((rows, half), BF16),
        ((2, sp * rs, HEAD_DIM), F32), ((2, stack[0], sp * rs), F32),
        ((2, sp, rs, HEAD_DIM), BF16), ((2, 3, rs, HEAD_DIM), BF16),
        ((tp, rs, kw), BF16), ((CORES, ny, tp, rs, kw), BF16), ((640,) + UNIT, BF16),
    ]
    return settled(pl.pallas_call(
        functools.partial(kernel, sp, tp),
        out_shape=(
            pltpu.VMEM((rows, width), BF16),
            pltpu.VMEM((source.shape[0], width), BF16),
            pltpu.VMEM(w_value.shape, F32),
        ),
        in_specs=[hbm] * 10,
        out_specs=(vmem,) * 3,
        scratch_shapes=[pltpu.VMEM(s, t) for s, t in scratch] + [
            dma((8,)), dma((3,)), dma((tp, ny)), dma((tp, 2)), dma((tp,)), dma((9,)),
        ],
        compiler_params=pltpu.CompilerParams(
            collective_id=0, has_side_effects=True, vmem_limit_bytes=VMEM_BYTES
        ),
    )(log_norm.T, keys, values, queries, attn_out, cotangent, source, w_query, w_key, w_value))


def shards(sp, tp, *args):
    queries, keys, source = args[0], args[4], args[6]
    if sp == 2 * CORES and tp == 4 * SIDE and queries.shape[0] == 128 and sp * keys.shape[0] == 128 and source.shape[0] == 256:
        return fused(sp, tp, *args)
    return plain(*args)


def plain(queries, attn_out, log_norm, cotangent, keys, values, source, w_query, w_key, w_value):
    single_precision = jnp.float32
    repeat = HEADS // KV_HEADS
    score_scale = 1.0 / math.sqrt(HEAD_DIM)
    rows = queries.shape[0]
    near_keys, near_values = (
        lax.all_gather(keys, "sp", axis=0, tiled=True),
        lax.all_gather(values, "sp", axis=0, tiled=True),
    )
    span = near_keys.shape[0]
    query_tensor4 = queries.reshape(rows, KV_HEADS, repeat, HEAD_DIM)
    output_gradient4 = cotangent.reshape(rows, KV_HEADS, repeat, HEAD_DIM)
    out4 = attn_out.reshape(rows, KV_HEADS, repeat, HEAD_DIM)
    shared_key_heads = near_keys.reshape(span, KV_HEADS, HEAD_DIM)
    shared_value_heads = near_values.reshape(span, KV_HEADS, HEAD_DIM)
    delta = jnp.sum(
        output_gradient4.astype(single_precision) * out4.astype(single_precision), axis=3
    )
    delta = jnp.transpose(delta, (1, 2, 0))[..., None]
    lse = jnp.transpose(log_norm.reshape(rows, KV_HEADS, repeat), (1, 2, 0))[..., None]
    logit_scores = (
        jnp.einsum(
            "znjk,wnk->njzw",
            query_tensor4,
            shared_key_heads,
            preferred_element_type=single_precision,
        )
        * score_scale
    )
    probs = jnp.exp(logit_scores - lse)
    probabilities16 = probs.astype(jnp.bfloat16)
    prob_gradient = jnp.einsum(
        "znjk,wnk->njzw",
        output_gradient4,
        shared_value_heads,
        preferred_element_type=single_precision,
    )
    score_gradient = (probs * (prob_gradient - delta)).astype(jnp.bfloat16)
    query_gradient_piece = (
        jnp.einsum(
            "wohn,nwb->hwob",
            score_gradient,
            shared_key_heads,
            preferred_element_type=single_precision,
        )
        * score_scale
    )
    query_gradient_piece = query_gradient_piece.reshape(rows, -1)
    key_gradient_piece = (
        jnp.einsum(
            "nkjv,jnka->vna", score_gradient, query_tensor4, preferred_element_type=single_precision
        )
        * score_scale
    )
    value_gradient_piece = jnp.einsum(
        "nkjv,jnka->vna", probabilities16, output_gradient4, preferred_element_type=single_precision
    )
    own_keys, own_values = (
        lax.psum_scatter(
            key_gradient_piece.reshape(span, -1).astype(jnp.bfloat16),
            "sp",
            scatter_dimension=0,
            tiled=True,
        ).astype(jnp.float32),
        lax.psum_scatter(
            value_gradient_piece.reshape(span, -1).astype(jnp.bfloat16),
            "sp",
            scatter_dimension=0,
            tiled=True,
        ).astype(jnp.float32),
    )
    stacked = jnp.concatenate(
        [own_keys.astype(jnp.bfloat16), own_values.astype(jnp.bfloat16)], axis=1
    )
    group = lax.all_gather(stacked, "tp", axis=0, tiled=True)
    weights = jnp.concatenate([w_key, w_value], axis=1)
    d_source = lax.dot_general(
        group, weights, (((1,), (1,)), ((), ())), preferred_element_type=single_precision
    ).astype(jnp.bfloat16)
    kv_width = w_value.shape[1]
    weight_term = lax.dot_general(
        source,
        group[:, kv_width:],
        (((0,), (0,)), ((), ())),
        preferred_element_type=single_precision,
    )
    d_wvalue = lax.psum(weight_term.astype(jnp.bfloat16), "sp").astype(jnp.float32)
    dq16 = lax.psum(query_gradient_piece, "tp").astype(jnp.bfloat16)
    d_target = lax.dot_general(
        dq16, w_query, (((1,), (1,)), ((), ())), preferred_element_type=single_precision
    ).astype(jnp.bfloat16)
    return (d_target, d_source, d_wvalue)


def solution(mesh):
    body = functools.partial(shards, mesh.shape["sp"], mesh.shape["tp"])
    in_specs = (
        P("sp", None),
        P("sp", None),
        P("sp", None),
        P("sp", None),
        P(("sp", "tp"), None),
        P(("sp", "tp"), None),
        P("sp", "tp"),
        P("tp", None),
        P("tp", None),
        P("tp", None),
    )
    out_specs = (P("sp", "tp"), P("sp", "tp"), P("tp", None))
    return jax.shard_map(body, mesh=mesh, in_specs=in_specs, out_specs=out_specs, check_vma=False)
```

```python
import functools
import math

import jax
import jax.numpy as jnp
from jax import lax
from jax.experimental import pallas as pl
from jax.experimental.pallas import tpu as pltpu
from jax.sharding import PartitionSpec as P

HEADS = 12
KV_HEADS = 2
HEAD_DIM = 256
CORES = 2
SIDE = 2
VMEM_BYTES = 64880640
UNIT = (16, 256)
MESH = pl.DeviceIdType.MESH
NT = (((1,), (1,)), ((), ()))
TN = (((0,), (0,)), ((), ()))
F32 = jnp.float32
BF16 = jnp.bfloat16


def dot(a, b, dims=(((1,), (0,)), ((), ()))):
    return lax.dot_general(a, b, dims, preferred_element_type=F32)


def kernel(
    sp, tp, lse_hbm, k_hbm, v_hbm, q_hbm, o_hbm, do_hbm, src_hbm, wq_hbm, wk_hbm, wv_hbm,
    dt_ref, ds_ref, src_t, dvf,
    kv, kvs, att, attr, wq, wk, wv, wqt, wkt, wvt, src, lsev, lse, delta, dqa, dq16, dqs, acc, prob,
    part, got, dkf, units,
    load_sem, send_sem, kv_recv, g_recv, gy_recv, one_recv,
):
    rows = q_hbm.shape[0]
    rs, kw = k_hbm.shape
    repeat = HEADS // KV_HEADS
    scale = 1.0 / math.sqrt(HEAD_DIM)
    log2e = math.log2(math.e)
    unit = UNIT[0] * UNIT[1] * 2
    i, j = lax.axis_index("sp"), lax.axis_index("tp")
    nz = tp // SIDE
    y, c = i // CORES, lax.rem(i, CORES)
    z, x = j // SIDE, lax.rem(j, SIDE)
    oy, oc, ox = 1 - y, 1 - c, 1 - x
    orders = [sorted((b for b in range(nz) if b != a), key=lambda b, a=a: abs(a - b)) for a in range(nz)]
    zs = [sum(jnp.where(z == a, order[n], 0) for a, order in enumerate(orders)) for n in range(nz - 1)]
    mid = (z == 1) | (z == 2)
    edge = jnp.where(z == 1, 0, 3)
    jx = z * SIDE + ox
    mine = [a * SIDE + x for a in zs]
    far = [a * SIDE + ox for a in zs]
    at_pair = (y * CORES + oc, j)
    at_y = (oy * CORES + c, j)
    at_x = (i, jx)
    sent = [0, 0]

    def bytes_of(ref):
        return math.prod(ref.shape) * jnp.dtype(ref.dtype).itemsize

    def send(a, b, r, device, s=0):
        pltpu.make_async_remote_copy(
            src_ref=a, dst_ref=b, send_sem=send_sem.at[s % 3], recv_sem=r, device_id=device, device_id_type=MESH,
        ).start()
        if s < 2:
            sent[s] += bytes_of(a)

    def receive(ref, r):
        pltpu.make_async_remote_copy(
            src_ref=ref, dst_ref=ref, send_sem=send_sem.at[0], recv_sem=r, device_id=at_pair, device_id_type=MESH,
        ).wait_recv()

    def load(a, b, s):
        pltpu.make_async_copy(a, b, load_sem.at[s]).start()
        return bytes_of(b)

    def take(size, s):
        ref = units.at[pl.ds(0, size // unit)]
        pltpu.make_async_copy(ref, ref, load_sem.at[s]).wait()

    own = pl.ds(pl.multiple_of(i * rs, rs), rs)
    theirs = pl.ds(pl.multiple_of((y * CORES + oc) * rs, rs), rs)
    kv_size = 0
    for t, r in enumerate((k_hbm, v_hbm)):
        for g in range(KV_HEADS):
            kv_size += load(r.at[:, pl.ds(g * HEAD_DIM, HEAD_DIM)], kvs.at[t, g], 0)
        kv_size += load(r.at[:, pl.ds(pl.multiple_of(c * HEAD_DIM, HEAD_DIM), HEAD_DIM)], kv.at[t, j, own], 0)
    barrier = pltpu.get_barrier_semaphore()

    def signal(device):
        pl.semaphore_signal(barrier, inc=1, device_id=device, device_id_type=MESH)

    near = [at_pair]
    for g in range(CORES):
        near += [(oy * CORES + g, j), (y * CORES + g, jx), (y * CORES + g, mine[0]), (y * CORES + g, mine[1])]
    for d in near:
        signal(d)

    @pl.when(mid)
    def _():
        for g in range(CORES):
            signal((y * CORES + g, mine[2]))

    def load_heads(g, a, r, s):
        size = 0
        for h in range(repeat):
            columns = pl.ds(pl.multiple_of((g * repeat + h) * HEAD_DIM, HEAD_DIM), HEAD_DIM)
            size += load(r.at[:, columns], att.at[a, g, pl.ds(h * rows, rows)], s)
        return size

    attn = (q_hbm, do_hbm, o_hbm)
    head_size = [load_heads(oc, a, r, 1 + a) for a, r in enumerate(attn)][0]
    own_size = sum(load_heads(c, a, r, 4) for a, r in enumerate(attn))
    load(lse_hbm, lsev.at[0], 5)
    src_size = load(src_hbm, src.at[c, y], 6)
    weight_size = load(wk_hbm, wk, 7) + load(wv_hbm, wv, 7)
    weight_size += load(wq_hbm, wq, 7)
    take(kv_size, 0)
    pl.semaphore_wait(barrier, len(near) + 2 * mid.astype(jnp.int32))


    def raw(y_to, slot, s=0):
        for g in range(CORES):
            send(kvs.at[:, g], kv.at[:, j, own], kv_recv.at[j, y], (y_to * CORES + g, slot), s)

    for t in range(2):
        for g in range(CORES):
            to = (oy * CORES + g, j)
            send(kvs.at[t, g], kv.at[t, j, own], kv_recv.at[j, y] if t == 0 else one_recv.at[9], to)
        send(kvs.at[t, oc], kv.at[t, j, own], kv_recv.at[j, y] if t == 0 else one_recv.at[10], at_pair)
    raw(y, jx)
    raw(y, mine[0])
    raw(y, mine[1])

    @pl.when(mid)
    def _():
        raw(y, mine[2], 1)

    def src_send(first):
        ref = src.at[c, y, pl.ds(0, cut) if first else pl.ds(cut, src.shape[2] - cut)]
        send(ref, ref, one_recv.at[3], at_y)

    cut = src.shape[2] * 5 // 8
    for a in range(3):
        take(head_size, 1 + a)
        send(att.at[a, oc], attr.at[a], one_recv.at[0 if a < 2 else 7], at_pair)
    pltpu.make_async_copy(lse_hbm, lsev.at[0], load_sem.at[5]).wait()
    send(lsev.at[0], lsev.at[1], one_recv.at[1], at_pair, 2)
    take(own_size, 4)
    take(src_size, 6)
    src_send(True)
    send(src.at[c, y], src.at[c, y], one_recv.at[4], at_pair)

    def block(b, a):
        return att[a, c] if b == 0 else attr[a]

    def deltas(b):
        for h in range(repeat):
            at = pl.ds(h * rows, rows)
            do, o = (att[a, c, at] if b == 0 else attr[a, at] for a in (1, 2))
            d = jnp.sum(do.astype(F32) * o.astype(F32), axis=1, keepdims=True)
            delta[b, at] = jnp.broadcast_to(d, (rows, 128))

    def norms(b):
        for h in range(repeat):
            row = jnp.where(c == 0, lsev[b, h:h + 1, :], lsev[b, repeat + h:repeat + h + 1, :])
            lse[b, pl.ds(h * rows, rows)] = jnp.transpose(jnp.broadcast_to(row * log2e, (128, rows)))

    norms(0)
    deltas(0)
    take(weight_size, 7)
    for n in range(repeat):
        columns = slice(n * kw, (n + 1) * kw)
        wqt[columns, :] = jnp.transpose(wq[:, columns])
    wkt[...] = jnp.transpose(wk[...])
    wvt[...] = jnp.transpose(wv[...])

    def piece(slot, h):
        return kv.at[:, slot, pl.ds(pl.multiple_of(h * (CORES * rs), CORES * rs), CORES * rs)]

    def arrived(slot, h):
        receive(piece(slot, h), kv_recv.at[slot, h])

    def relay(slot, h, device, s=0):
        send(piece(slot, h), piece(slot, h), kv_recv.at[slot, h], device, s)

    def from_z(n, h, s=0):
        arrived(mine[n], h)
        relay(mine[n], h, at_x, s)

    def half_piece(t):
        return kv.at[t, j, pl.ds(pl.multiple_of(oy * (CORES * rs), CORES * rs), CORES * rs)]

    def along_z(t):
        def one(device, s=0):
            send(half_piece(t), half_piece(t), kv_recv.at[j, oy], device, s)

        one((i, mine[0]))
        one(at_x)

        @pl.when(mid)
        def _():
            one((i, mine[1]), 1)
            one((i, mine[2]), 1)

    receive(kv.at[0, j, theirs], kv_recv.at[j, y])
    receive(half_piece(0), kv_recv.at[j, oy])
    along_z(0)
    receive(attr.at[pl.ds(0, 2)], one_recv.at[0])
    receive(lsev.at[1], one_recv.at[1])
    norms(1)

    def wide(a, n):
        return a if n == 1 else jnp.concatenate([a] * n, axis=1)

    def probs(b, keys):
        return jnp.exp2(dot(block(b, 0), keys, NT) * (scale * log2e) - wide(lse[b], keys.shape[0] // 128))

    def scores(b, p, values):
        dp = dot(block(b, 1), values, NT)
        return (p * (dp - wide(delta[b], values.shape[0] // 128))).astype(BF16)

    def part_send(t, r):
        for g in range(CORES):
            to = oy * CORES + g
            send(part.at[t, to], got.at[t, 1 + c], r, (to, j))
        send(part.at[t, y * CORES + oc], got.at[t, 0], r, at_pair)

    for b in range(2):
        p = probs(b, kv[0, j])
        prob[b] = p
        dv = dot(p.astype(BF16), block(b, 1), TN)
        if b == 0:
            acc[1] = dv
        else:
            part[1] = (acc[1] + dv).astype(BF16).reshape(sp, rs, HEAD_DIM)
    part_send(1, one_recv.at[2])
    receive(kv.at[1, j, theirs], one_recv.at[10])
    receive(half_piece(1), one_recv.at[9])
    along_z(1)
    from_z(0, y)
    receive(attr.at[2], one_recv.at[7])
    deltas(1)
    for b in range(2):
        keys = kv[0, j]
        ds = scores(b, prob[b], kv[1, j])
        dk = dot(ds, block(b, 0), TN)
        dqa[b] = dot(ds, keys)
        if b == 0:
            acc[0] = dk

            @pl.when(mid)
            def _():
                arrived(mine[1], y)
                relay(mine[1], y, at_x, 3)
                arrived(mine[2], y)
                relay(mine[2], y, (i, edge * SIDE + x), 1)
                relay(mine[2], y, at_y, 3)

        else:
            part[0] = ((acc[0] + dk) * scale).astype(BF16).reshape(sp, rs, HEAD_DIM)
    part_send(0, one_recv.at[8])
    src_send(False)

    def chunk(slots, order=(0, 1)):
        for b in order:
            keys, values = (kv[t, slots].reshape(-1, HEAD_DIM) for t in range(2))
            dqa[b] += dot(scores(b, probs(b, keys), values), keys)

    def total(t):
        here = part[t, i].astype(F32) + got[t, 1 + c].astype(F32)
        there = got[t, 0].astype(F32) + got[t, 1 + oc].astype(F32)
        ref = dkf.at[j] if t == 0 else dvf.at[c, y, j]
        for g in range(KV_HEADS):
            ref[:, g * HEAD_DIM:(g + 1) * HEAD_DIM] = jnp.where(c == g, here, there).astype(BF16)

    def grad(t, slot):
        return dkf.at[slot] if t == 0 else dvf.at[c, y, slot]

    def g_send(t, slot, device, s=0):
        send(grad(t, slot), grad(t, slot), g_recv.at[slot, t], device, s)

    def g_arrived(t, slot):
        receive(grad(t, slot), g_recv.at[slot, t])

    def g_along_z(t, slot):
        g_send(t, slot, (i, mine[0]))
        g_send(t, slot, (i, mine[1]))
        pl.when(mid)(lambda: g_send(t, slot, (i, mine[2]), 1 if t == 1 else 3))
        if t == 0:
            sent[0] += bytes_of(grad(t, slot))

    def g_spread(slot, last=False, s=0):
        ref = grad(1, slot)
        send(ref, ref, gy_recv.at[slot], at_y, s)
        send(ref, ref, one_recv.at[5], at_pair, s)
        if last:
            send(ref, ref, one_recv.at[5], (oy * CORES + oc, j), s)

    def g_from_y(slot, last=False):
        ref = dvf.at[c, oy, slot]
        receive(ref, gy_recv.at[slot])
        if not last:
            send(ref, ref, one_recv.at[5], at_pair)

    def dv_from(slot):
        g_arrived(1, slot)
        g_spread(slot)

    def dv_last(slot, early, last=False):
        def body():
            g_arrived(1, slot)
            if early:
                g_send(1, slot, (i, edge * SIDE + x), 1)
            g_spread(slot, last, 0 if early else 3)

        pl.when(mid if early else jnp.logical_not(mid))(body)

    def dk_from(n):
        g_arrived(0, mine[n])
        g_send(0, mine[n], at_x)

    def chunk_z(n, order=(0, 1)):
        chunk(pl.ds(zs[n] * SIDE, SIDE), order)

    def far_arrived(n):
        arrived(far[n], y)
        arrived(far[n], oy)

    receive(got.at[1], one_recv.at[2])
    total(1)
    g_send(1, j, at_x)
    g_along_z(1, j)
    g_spread(j)

    @pl.when(mid)
    def _():
        relay(mine[2], y, at_x, 3)

    @pl.when(jnp.logical_not(mid))
    def _():
        arrived(mine[1], y)
        relay(mine[1], y, at_x)

    sent[0] += 2 * bytes_of(piece(mine[2], y))
    from_z(0, oy)
    pl.when(mid)(lambda: from_z(2, oy, 3))
    arrived(jx, y)
    arrived(jx, oy)
    chunk(pl.ds(jx, 1))
    receive(got.at[0], one_recv.at[8])
    total(0)
    g_along_z(0, j)
    pl.when(jnp.logical_not(mid))(lambda: g_send(0, j, (i, mine[2]), 3))
    g_send(0, j, at_x)
    from_z(1, oy)
    g_arrived(1, jx)
    g_along_z(1, jx)
    g_spread(jx)

    @pl.when(jnp.logical_not(mid))
    def _():
        arrived(mine[2], y)
        relay(mine[2], y, at_y, 3)
        relay(mine[2], y, at_x, 3)

    dv_from(mine[0])
    dv_last(mine[2], True)
    far_arrived(0)
    chunk_z(0)
    pl.when(jnp.logical_not(mid))(lambda: from_z(2, oy))
    dv_from(mine[1])
    dv_from(far[0])
    dv_last(far[2], True, True)
    far_arrived(1)
    chunk_z(1)
    dv_last(mine[2], False)
    dk_from(0)
    dk_from(1)
    receive(src.at[c, oy], one_recv.at[3])
    send(src.at[c, oy], src.at[c, oy], one_recv.at[4], at_pair)
    g_from_y(j)
    g_from_y(jx)
    dv_from(far[1])
    dk_from(2)
    far_arrived(2)
    chunk_z(2, (1,))

    def rounded(b, ref):
        for h in range(repeat):
            ref[:, h * HEAD_DIM:(h + 1) * HEAD_DIM] = (dqa[b, h * rows:(h + 1) * rows] * scale).astype(BF16)

    half = dqs.shape[1]
    rounded(1, dqs)
    send(dqs, dq16.at[:, pl.ds(pl.multiple_of(c * half, half), half)], one_recv.at[6], at_pair)
    dv_last(far[2], False, True)
    chunk_z(2, (0,))
    for h in range(repeat):
        at = pl.ds(pl.multiple_of(c * half + h * HEAD_DIM, HEAD_DIM), HEAD_DIM)
        dq16[:, at] = (dqa[0, h * rows:(h + 1) * rows] * scale).astype(BF16)
    receive(src.at[oc], one_recv.at[4])
    deep = src.shape[2]
    for b in range(sp // CORES):
        for a in range(CORES):
            n = b * CORES + a
            src_t[:, n * deep:(n + 1) * deep] = jnp.transpose(src[a, b])
    for slot in [mine[0], mine[1], far[0], mine[2], far[1]]:
        g_from_y(slot)
    receive(dq16.at[:, pl.ds(pl.multiple_of(oc * half, half), half)], one_recv.at[6])
    dt_ref[...] = dot(dq16[...], wqt[...]).astype(BF16)
    g_arrived(0, jx)
    for n in range(nz - 1):
        g_arrived(0, far[n])
    ds_ref[...] = (
        dot(dkf[...].reshape(-1, kw), wkt[...]) + dot(dvf[c, y].reshape(-1, kw), wvt[...])
    ).astype(BF16)
    g_from_y(far[2], True)
    receive(dvf.at[oc], one_recv.at[5])

    def sent_all(s):
        ref = units.at[pl.ds(0, sent[s] // unit)]
        pltpu.make_async_remote_copy(
            src_ref=ref, dst_ref=ref, send_sem=send_sem.at[s], recv_sem=one_recv.at[0],
            device_id=at_pair, device_id_type=MESH,
        ).wait_send()

    sent_all(0)
    pl.when(mid)(lambda: sent_all(1))
    pltpu.make_async_remote_copy(
        src_ref=lsev.at[0], dst_ref=lsev.at[1], send_sem=send_sem.at[2], recv_sem=one_recv.at[1],
        device_id=at_pair, device_id_type=MESH,
    ).wait_send()


def finish(dt_ref, ds_ref, src_t, dvf, dt_hbm, ds_hbm, dw_hbm, dw_ref, sems):
    small = [
        pltpu.make_async_copy(a, b, sems.at[n]) for n, (a, b) in enumerate(((dt_ref, dt_hbm), (ds_ref, ds_hbm)))
    ]
    for copy in small:
        copy.start()
    kw = dw_ref.shape[1]
    dv = jnp.concatenate(
        [dvf[a, b].reshape(-1, kw) for b in range(dvf.shape[1]) for a in range(CORES)], axis=0)
    pieces = 3
    tall = dw_ref.shape[0] // pieces
    for n in range(pieces):
        at = pl.ds(n * tall, tall)
        dw_ref[at] = dot(src_t[at], dv)
        copy = pltpu.make_async_copy(dw_ref.at[at], dw_hbm.at[at], sems.at[2 + n])
        copy.start()
        small.append(copy)
    for copy in small:
        copy.wait()


def finished(shape, dt, ds, src_t, dvf):
    vmem, hbm = pl.BlockSpec(memory_space=pltpu.VMEM), pl.BlockSpec(memory_space=pl.ANY)
    return pl.pallas_call(
        finish,
        out_shape=(
            jax.ShapeDtypeStruct(dt.shape, BF16), jax.ShapeDtypeStruct(ds.shape, BF16), jax.ShapeDtypeStruct(shape, F32),
        ),
        in_specs=[vmem] * 4,
        out_specs=(hbm,) * 3,
        scratch_shapes=[pltpu.VMEM(shape, F32), pltpu.SemaphoreType.DMA((5,))],
        compiler_params=pltpu.CompilerParams(vmem_limit_bytes=16 * 1024 * 1024),
    )(dt, ds, src_t, dvf)


def fused(sp, tp, queries, attn_out, log_norm, cotangent, keys, values, source, w_query, w_key, w_value):
    rows, model = queries.shape
    width = w_value.shape[0]
    rs, kw = keys.shape
    vmem, hbm = pl.BlockSpec(memory_space=pltpu.VMEM), pl.BlockSpec(memory_space=pl.ANY)
    dma = pltpu.SemaphoreType.DMA
    stack = (rows * HEADS // KV_HEADS, HEAD_DIM)
    half = model // KV_HEADS
    ny = sp // CORES
    scratch = [
        ((2, tp, sp * rs, HEAD_DIM), BF16), ((2, KV_HEADS, rs, HEAD_DIM), BF16),
        ((3, KV_HEADS) + stack, BF16), ((3,) + stack, BF16),
        (w_query.shape, BF16), (w_key.shape, BF16), (w_value.shape, BF16),
        (w_query.shape[::-1], BF16), (w_key.shape[::-1], BF16), (w_value.shape[::-1], BF16),
        ((CORES, ny) + source.shape, BF16),
        ((2, HEADS, rows), F32), ((2, stack[0], 128), F32), ((2, stack[0], 128), F32),
        ((2,) + stack, F32), ((rows, model), BF16), ((rows, half), BF16),
        ((2, sp * rs, HEAD_DIM), F32), ((2, stack[0], sp * rs), F32),
        ((2, sp, rs, HEAD_DIM), BF16), ((2, 3, rs, HEAD_DIM), BF16),
        ((tp, rs, kw), BF16), ((640,) + UNIT, BF16),
    ]
    return finished(w_value.shape, *pl.pallas_call(
        functools.partial(kernel, sp, tp),
        out_shape=(
            pltpu.VMEM((rows, width), BF16),
            pltpu.VMEM((source.shape[0], width), BF16),
            pltpu.VMEM((width, sp * source.shape[0]), BF16),
            pltpu.VMEM((CORES, ny, tp, rs, kw), BF16),
        ),
        in_specs=[hbm] * 10,
        out_specs=(vmem,) * 4,
        scratch_shapes=[pltpu.VMEM(s, t) for s, t in scratch] + [
            dma((8,)), dma((3,)), dma((tp, ny)), dma((tp, 2)), dma((tp,)), dma((11,)),
        ],
        compiler_params=pltpu.CompilerParams(
            collective_id=0, has_side_effects=True, vmem_limit_bytes=VMEM_BYTES
        ),
    )(log_norm.T, keys, values, queries, attn_out, cotangent, source, w_query, w_key, w_value))


def shards(sp, tp, *args):
    queries, keys, source = args[0], args[4], args[6]
    if sp == 2 * CORES and tp == 4 * SIDE and queries.shape[0] == 128 and sp * keys.shape[0] == 128 and source.shape[0] == 256:
        return fused(sp, tp, *args)
    return plain(*args)


def plain(queries, attn_out, log_norm, cotangent, keys, values, source, w_query, w_key, w_value):
    single_precision = jnp.float32
    repeat = HEADS // KV_HEADS
    score_scale = 1.0 / math.sqrt(HEAD_DIM)
    rows = queries.shape[0]
    near_keys, near_values = (
        lax.all_gather(keys, "sp", axis=0, tiled=True),
        lax.all_gather(values, "sp", axis=0, tiled=True),
    )
    span = near_keys.shape[0]
    query_tensor4 = queries.reshape(rows, KV_HEADS, repeat, HEAD_DIM)
    output_gradient4 = cotangent.reshape(rows, KV_HEADS, repeat, HEAD_DIM)
    out4 = attn_out.reshape(rows, KV_HEADS, repeat, HEAD_DIM)
    shared_key_heads = near_keys.reshape(span, KV_HEADS, HEAD_DIM)
    shared_value_heads = near_values.reshape(span, KV_HEADS, HEAD_DIM)
    delta = jnp.sum(
        output_gradient4.astype(single_precision) * out4.astype(single_precision), axis=3
    )
    delta = jnp.transpose(delta, (1, 2, 0))[..., None]
    lse = jnp.transpose(log_norm.reshape(rows, KV_HEADS, repeat), (1, 2, 0))[..., None]
    logit_scores = (
        jnp.einsum(
            "znjk,wnk->njzw",
            query_tensor4,
            shared_key_heads,
            preferred_element_type=single_precision,
        )
        * score_scale
    )
    probs = jnp.exp(logit_scores - lse)
    probabilities16 = probs.astype(jnp.bfloat16)
    prob_gradient = jnp.einsum(
        "znjk,wnk->njzw",
        output_gradient4,
        shared_value_heads,
        preferred_element_type=single_precision,
    )
    score_gradient = (probs * (prob_gradient - delta)).astype(jnp.bfloat16)
    query_gradient_piece = (
        jnp.einsum(
            "wohn,nwb->hwob",
            score_gradient,
            shared_key_heads,
            preferred_element_type=single_precision,
        )
        * score_scale
    )
    query_gradient_piece = query_gradient_piece.reshape(rows, -1)
    key_gradient_piece = (
        jnp.einsum(
            "nkjv,jnka->vna", score_gradient, query_tensor4, preferred_element_type=single_precision
        )
        * score_scale
    )
    value_gradient_piece = jnp.einsum(
        "nkjv,jnka->vna", probabilities16, output_gradient4, preferred_element_type=single_precision
    )
    own_keys, own_values = (
        lax.psum_scatter(
            key_gradient_piece.reshape(span, -1).astype(jnp.bfloat16),
            "sp",
            scatter_dimension=0,
            tiled=True,
        ).astype(jnp.float32),
        lax.psum_scatter(
            value_gradient_piece.reshape(span, -1).astype(jnp.bfloat16),
            "sp",
            scatter_dimension=0,
            tiled=True,
        ).astype(jnp.float32),
    )
    stacked = jnp.concatenate(
        [own_keys.astype(jnp.bfloat16), own_values.astype(jnp.bfloat16)], axis=1
    )
    group = lax.all_gather(stacked, "tp", axis=0, tiled=True)
    weights = jnp.concatenate([w_key, w_value], axis=1)
    d_source = lax.dot_general(
        group, weights, (((1,), (1,)), ((), ())), preferred_element_type=single_precision
    ).astype(jnp.bfloat16)
    kv_width = w_value.shape[1]
    weight_term = lax.dot_general(
        source,
        group[:, kv_width:],
        (((0,), (0,)), ((), ())),
        preferred_element_type=single_precision,
    )
    d_wvalue = lax.psum(weight_term.astype(jnp.bfloat16), "sp").astype(jnp.float32)
    dq16 = lax.psum(query_gradient_piece, "tp").astype(jnp.bfloat16)
    d_target = lax.dot_general(
        dq16, w_query, (((1,), (1,)), ((), ())), preferred_element_type=single_precision
    ).astype(jnp.bfloat16)
    return (d_target, d_source, d_wvalue)


def solution(mesh):
    body = functools.partial(shards, mesh.shape["sp"], mesh.shape["tp"])
    in_specs = (
        P("sp", None),
        P("sp", None),
        P("sp", None),
        P("sp", None),
        P(("sp", "tp"), None),
        P(("sp", "tp"), None),
        P("sp", "tp"),
        P("tp", None),
        P("tp", None),
        P("tp", None),
    )
    out_specs = (P("sp", "tp"), P("sp", "tp"), P("tp", None))
    return jax.shard_map(body, mesh=mesh, in_specs=in_specs, out_specs=out_specs, check_vma=False)
```

```python
import functools
import math

import jax
import jax.numpy as jnp
from jax import lax
from jax.experimental import pallas as pl
from jax.experimental.pallas import tpu as pltpu
from jax.sharding import PartitionSpec as P

HEADS = 12
KV_HEADS = 2
HEAD_DIM = 256
CORES = 2
SIDE = 2
VMEM_BYTES = 64880640
UNIT = (16, 256)
MESH = pl.DeviceIdType.MESH
NT = (((1,), (1,)), ((), ()))
TN = (((0,), (0,)), ((), ()))
F32 = jnp.float32
BF16 = jnp.bfloat16


def dot(a, b, dims=(((1,), (0,)), ((), ()))):
    return lax.dot_general(a, b, dims, preferred_element_type=F32)


def kernel(
    sp, tp, lse_hbm, k_hbm, v_hbm, q_hbm, o_hbm, do_hbm, src_hbm, wq_hbm, wk_hbm, wv_hbm,
    dt_ref, ds_ref, src_t, dvf,
    kv, kvs, att, attr, wq, wk, wv, wqt, wkt, wvt, src, lsev, lse, delta, dqa, dq16, dqs, acc, prob,
    part, got, dkf, units,
    load_sem, send_sem, kv_recv, g_recv, gy_recv, one_recv,
):
    rows = q_hbm.shape[0]
    rs, kw = k_hbm.shape
    repeat = HEADS // KV_HEADS
    scale = 1.0 / math.sqrt(HEAD_DIM)
    log2e = math.log2(math.e)
    unit = UNIT[0] * UNIT[1] * 2
    i, j = lax.axis_index("sp"), lax.axis_index("tp")
    nz = tp // SIDE
    y, c = i // CORES, lax.rem(i, CORES)
    z, x = j // SIDE, lax.rem(j, SIDE)
    oy, oc, ox = 1 - y, 1 - c, 1 - x
    orders = [sorted((b for b in range(nz) if b != a), key=lambda b, a=a: abs(a - b)) for a in range(nz)]
    zs = [sum(jnp.where(z == a, order[n], 0) for a, order in enumerate(orders)) for n in range(nz - 1)]
    mid = (z == 1) | (z == 2)
    edge = jnp.where(z == 1, 0, 3)
    jx = z * SIDE + ox
    mine = [a * SIDE + x for a in zs]
    far = [a * SIDE + ox for a in zs]
    at_pair = (y * CORES + oc, j)
    at_y = (oy * CORES + c, j)
    at_x = (i, jx)
    sent = [0, 0]

    def bytes_of(ref):
        return math.prod(ref.shape) * jnp.dtype(ref.dtype).itemsize

    def send(a, b, r, device, s=0):
        pltpu.make_async_remote_copy(
            src_ref=a, dst_ref=b, send_sem=send_sem.at[s % 3], recv_sem=r, device_id=device, device_id_type=MESH,
        ).start()
        if s < 2:
            sent[s] += bytes_of(a)

    def receive(ref, r):
        pltpu.make_async_remote_copy(
            src_ref=ref, dst_ref=ref, send_sem=send_sem.at[0], recv_sem=r, device_id=at_pair, device_id_type=MESH,
        ).wait_recv()

    def load(a, b, s):
        pltpu.make_async_copy(a, b, load_sem.at[s]).start()
        return bytes_of(b)

    def take(size, s):
        ref = units.at[pl.ds(0, size // unit)]
        pltpu.make_async_copy(ref, ref, load_sem.at[s]).wait()

    own = pl.ds(pl.multiple_of(i * rs, rs), rs)
    theirs = pl.ds(pl.multiple_of((y * CORES + oc) * rs, rs), rs)
    kv_size = 0
    for t, r in enumerate((k_hbm, v_hbm)):
        for g in range(KV_HEADS):
            kv_size += load(r.at[:, pl.ds(g * HEAD_DIM, HEAD_DIM)], kvs.at[t, g], 0)
        kv_size += load(r.at[:, pl.ds(pl.multiple_of(c * HEAD_DIM, HEAD_DIM), HEAD_DIM)], kv.at[t, j, own], 0)
    barrier = pltpu.get_barrier_semaphore()

    def signal(device):
        pl.semaphore_signal(barrier, inc=1, device_id=device, device_id_type=MESH)

    near = [at_pair]
    for g in range(CORES):
        near += [(oy * CORES + g, j), (y * CORES + g, jx), (y * CORES + g, mine[0]), (y * CORES + g, mine[1])]
    for d in near:
        signal(d)

    @pl.when(mid)
    def _():
        for g in range(CORES):
            signal((y * CORES + g, mine[2]))

    def load_heads(g, a, r, s):
        size = 0
        for h in range(repeat):
            columns = pl.ds(pl.multiple_of((g * repeat + h) * HEAD_DIM, HEAD_DIM), HEAD_DIM)
            size += load(r.at[:, columns], att.at[a, g, pl.ds(h * rows, rows)], s)
        return size

    attn = (q_hbm, do_hbm, o_hbm)
    head_size = [load_heads(oc, a, r, 1 + a) for a, r in enumerate(attn)][0]
    own_size = sum(load_heads(c, a, r, 4) for a, r in enumerate(attn))
    load(lse_hbm, lsev.at[0], 5)
    src_size = load(src_hbm, src.at[c, y], 6)
    weight_size = load(wk_hbm, wk, 7) + load(wv_hbm, wv, 7)
    weight_size += load(wq_hbm, wq, 7)
    take(kv_size, 0)
    pl.semaphore_wait(barrier, len(near) + 2 * mid.astype(jnp.int32))


    def raw(y_to, slot, s=0):
        for g in range(CORES):
            send(kvs.at[:, g], kv.at[:, j, own], kv_recv.at[j, y], (y_to * CORES + g, slot), s)

    for t in range(2):
        for g in range(CORES):
            to = (oy * CORES + g, j)
            send(kvs.at[t, g], kv.at[t, j, own], kv_recv.at[j, y] if t == 0 else one_recv.at[9], to)
        send(kvs.at[t, oc], kv.at[t, j, own], kv_recv.at[j, y] if t == 0 else one_recv.at[10], at_pair)
    raw(y, jx)
    raw(y, mine[0])
    raw(y, mine[1])

    @pl.when(mid)
    def _():
        raw(y, mine[2], 1)

    def src_send(first):
        ref = src.at[c, y, pl.ds(0, cut) if first else pl.ds(cut, src.shape[2] - cut)]
        send(ref, ref, one_recv.at[3], at_y)

    cut = src.shape[2] * 5 // 8
    for a in range(3):
        take(head_size, 1 + a)
        send(att.at[a, oc], attr.at[a], one_recv.at[0 if a < 2 else 7], at_pair)
    pltpu.make_async_copy(lse_hbm, lsev.at[0], load_sem.at[5]).wait()
    send(lsev.at[0], lsev.at[1], one_recv.at[1], at_pair, 2)
    take(own_size, 4)
    take(src_size, 6)
    src_send(True)
    send(src.at[c, y], src.at[c, y], one_recv.at[4], at_pair)

    def block(b, a):
        return att[a, c] if b == 0 else attr[a]

    def deltas(b):
        for h in range(repeat):
            at = pl.ds(h * rows, rows)
            do, o = (att[a, c, at] if b == 0 else attr[a, at] for a in (1, 2))
            d = jnp.sum(do.astype(F32) * o.astype(F32), axis=1, keepdims=True)
            delta[b, at] = jnp.broadcast_to(d, (rows, 128))

    def norms(b):
        for h in range(repeat):
            row = jnp.where(c == 0, lsev[b, h:h + 1, :], lsev[b, repeat + h:repeat + h + 1, :])
            lse[b, pl.ds(h * rows, rows)] = jnp.transpose(jnp.broadcast_to(row * log2e, (128, rows)))

    norms(0)
    deltas(0)
    take(weight_size, 7)
    for n in range(repeat):
        columns = slice(n * kw, (n + 1) * kw)
        wqt[columns, :] = jnp.transpose(wq[:, columns])
    wkt[...] = jnp.transpose(wk[...])
    wvt[...] = jnp.transpose(wv[...])

    def piece(slot, h):
        return kv.at[:, slot, pl.ds(pl.multiple_of(h * (CORES * rs), CORES * rs), CORES * rs)]

    def arrived(slot, h):
        receive(piece(slot, h), kv_recv.at[slot, h])

    def relay(slot, h, device, s=0):
        send(piece(slot, h), piece(slot, h), kv_recv.at[slot, h], device, s)

    def from_z(n, h, s=0):
        arrived(mine[n], h)
        relay(mine[n], h, at_x, s)

    def half_piece(t):
        return kv.at[t, j, pl.ds(pl.multiple_of(oy * (CORES * rs), CORES * rs), CORES * rs)]

    def along_z(t):
        def one(device, s=0):
            send(half_piece(t), half_piece(t), kv_recv.at[j, oy], device, s)

        one((i, mine[0]))
        one(at_x)

        @pl.when(mid)
        def _():
            one((i, mine[1]), 1)
            one((i, mine[2]), 1)

    receive(kv.at[0, j, theirs], kv_recv.at[j, y])
    receive(half_piece(0), kv_recv.at[j, oy])
    along_z(0)
    receive(attr.at[pl.ds(0, 2)], one_recv.at[0])
    receive(lsev.at[1], one_recv.at[1])
    norms(1)

    def wide(a, n):
        return a if n == 1 else jnp.concatenate([a] * n, axis=1)

    def probs(b, keys):
        return jnp.exp2(dot(block(b, 0), keys, NT) * (scale * log2e) - wide(lse[b], keys.shape[0] // 128))

    def scores(b, p, values):
        dp = dot(block(b, 1), values, NT)
        return (p * (dp - wide(delta[b], values.shape[0] // 128))).astype(BF16)

    def part_send(t, r):
        for g in range(CORES):
            to = oy * CORES + g
            send(part.at[t, to], got.at[t, 1 + c], r, (to, j))
        send(part.at[t, y * CORES + oc], got.at[t, 0], r, at_pair)

    for b in range(2):
        p = probs(b, kv[0, j])
        prob[b] = p
        dv = dot(p.astype(BF16), block(b, 1), TN)
        if b == 0:
            acc[1] = dv
        else:
            part[1] = (acc[1] + dv).astype(BF16).reshape(sp, rs, HEAD_DIM)
    part_send(1, one_recv.at[2])
    receive(kv.at[1, j, theirs], one_recv.at[10])
    receive(half_piece(1), one_recv.at[9])
    along_z(1)
    from_z(0, y)
    receive(attr.at[2], one_recv.at[7])
    deltas(1)
    for b in range(2):
        keys = kv[0, j]
        ds = scores(b, prob[b], kv[1, j])
        dk = dot(ds, block(b, 0), TN)
        dqa[b] = dot(ds, keys)
        if b == 0:
            acc[0] = dk

            @pl.when(mid)
            def _():
                arrived(mine[1], y)
                relay(mine[1], y, at_x, 3)
                arrived(mine[2], y)
                relay(mine[2], y, (i, edge * SIDE + x), 1)
                relay(mine[2], y, at_y, 3)

        else:
            part[0] = ((acc[0] + dk) * scale).astype(BF16).reshape(sp, rs, HEAD_DIM)
    part_send(0, one_recv.at[8])
    src_send(False)

    def chunk(slots, order=(0, 1)):
        for b in order:
            keys, values = (kv[t, slots].reshape(-1, HEAD_DIM) for t in range(2))
            dqa[b] += dot(scores(b, probs(b, keys), values), keys)

    def total(t):
        here = part[t, i].astype(F32) + got[t, 1 + c].astype(F32)
        there = got[t, 0].astype(F32) + got[t, 1 + oc].astype(F32)
        ref = dkf.at[j] if t == 0 else dvf.at[c, y, j]
        for g in range(KV_HEADS):
            ref[:, g * HEAD_DIM:(g + 1) * HEAD_DIM] = jnp.where(c == g, here, there).astype(BF16)

    def grad(t, slot):
        return dkf.at[slot] if t == 0 else dvf.at[c, y, slot]

    def g_send(t, slot, device, s=0):
        send(grad(t, slot), grad(t, slot), g_recv.at[slot, t], device, s)

    def g_arrived(t, slot):
        receive(grad(t, slot), g_recv.at[slot, t])

    def g_along_z(t, slot):
        g_send(t, slot, (i, mine[0]))
        g_send(t, slot, (i, mine[1]))
        pl.when(mid)(lambda: g_send(t, slot, (i, mine[2]), 1 if t == 1 else 3))
        if t == 0:
            sent[0] += bytes_of(grad(t, slot))

    def g_spread(slot, last=False, s=0):
        ref = grad(1, slot)
        send(ref, ref, gy_recv.at[slot], at_y, s)
        send(ref, ref, one_recv.at[5], at_pair, s)
        if last:
            send(ref, ref, one_recv.at[5], (oy * CORES + oc, j), s)

    def g_from_y(slot, last=False):
        ref = dvf.at[c, oy, slot]
        receive(ref, gy_recv.at[slot])
        if not last:
            send(ref, ref, one_recv.at[5], at_pair)

    def dv_from(slot):
        g_arrived(1, slot)
        g_spread(slot)

    def dv_last(slot, early, last=False):
        def body():
            g_arrived(1, slot)
            if early:
                g_send(1, slot, (i, edge * SIDE + x), 1)
            g_spread(slot, last, 0 if early else 3)

        pl.when(mid if early else jnp.logical_not(mid))(body)

    def dk_from(n):
        g_arrived(0, mine[n])
        g_send(0, mine[n], at_x)

    def chunk_z(n, order=(0, 1)):
        chunk(pl.ds(zs[n] * SIDE, SIDE), order)

    def far_arrived(n):
        arrived(far[n], y)
        arrived(far[n], oy)

    receive(got.at[1], one_recv.at[2])
    total(1)
    g_send(1, j, at_x)
    g_along_z(1, j)
    g_spread(j)

    @pl.when(mid)
    def _():
        relay(mine[2], y, at_x, 3)

    @pl.when(jnp.logical_not(mid))
    def _():
        arrived(mine[1], y)
        relay(mine[1], y, at_x)

    sent[0] += 2 * bytes_of(piece(mine[2], y))
    from_z(0, oy)
    pl.when(mid)(lambda: from_z(2, oy, 3))
    arrived(jx, y)
    arrived(jx, oy)
    chunk(pl.ds(jx, 1))
    receive(got.at[0], one_recv.at[8])
    total(0)
    g_along_z(0, j)
    pl.when(jnp.logical_not(mid))(lambda: g_send(0, j, (i, mine[2]), 3))
    g_send(0, j, at_x)
    from_z(1, oy)
    g_arrived(1, jx)
    g_along_z(1, jx)
    g_spread(jx)

    @pl.when(jnp.logical_not(mid))
    def _():
        arrived(mine[2], y)
        relay(mine[2], y, at_y, 3)
        relay(mine[2], y, at_x, 3)

    dv_from(mine[0])
    dv_last(mine[2], True)
    far_arrived(0)
    chunk_z(0)
    pl.when(jnp.logical_not(mid))(lambda: from_z(2, oy))
    dv_from(mine[1])
    dv_from(far[0])
    dv_last(far[2], True, True)
    receive(src.at[c, oy], one_recv.at[3])
    send(src.at[c, oy], src.at[c, oy], one_recv.at[4], at_pair)
    far_arrived(1)
    chunk_z(1)
    dv_last(mine[2], False)
    dk_from(0)
    dk_from(1)
    g_from_y(j)
    g_from_y(jx)
    dv_from(far[1])
    dk_from(2)
    receive(src.at[oc], one_recv.at[4])
    deep = src.shape[2]
    for b in range(sp // CORES):
        for a in range(CORES):
            n = b * CORES + a
            src_t[:, n * deep:(n + 1) * deep] = jnp.transpose(src[a, b])
    far_arrived(2)
    dv_last(far[2], False, True)
    chunk_z(2, (1,))

    def rounded(b, ref):
        for h in range(repeat):
            ref[:, h * HEAD_DIM:(h + 1) * HEAD_DIM] = (dqa[b, h * rows:(h + 1) * rows] * scale).astype(BF16)

    half = dqs.shape[1]
    rounded(1, dqs)
    send(dqs, dq16.at[:, pl.ds(pl.multiple_of(c * half, half), half)], one_recv.at[6], at_pair)
    chunk_z(2, (0,))
    for h in range(repeat):
        at = pl.ds(pl.multiple_of(c * half + h * HEAD_DIM, HEAD_DIM), HEAD_DIM)
        dq16[:, at] = (dqa[0, h * rows:(h + 1) * rows] * scale).astype(BF16)
    for slot in [mine[0], mine[1], far[0], mine[2], far[1]]:
        g_from_y(slot)
    receive(dq16.at[:, pl.ds(pl.multiple_of(oc * half, half), half)], one_recv.at[6])
    dt_ref[...] = dot(dq16[...], wqt[...]).astype(BF16)
    g_arrived(0, jx)
    for n in range(nz - 1):
        g_arrived(0, far[n])
    ds_ref[...] = (
        dot(dkf[...].reshape(-1, kw), wkt[...]) + dot(dvf[c, y].reshape(-1, kw), wvt[...])
    ).astype(BF16)
    g_from_y(far[2], True)
    receive(dvf.at[oc], one_recv.at[5])

    def sent_all(s):
        ref = units.at[pl.ds(0, sent[s] // unit)]
        pltpu.make_async_remote_copy(
            src_ref=ref, dst_ref=ref, send_sem=send_sem.at[s], recv_sem=one_recv.at[0],
            device_id=at_pair, device_id_type=MESH,
        ).wait_send()

    sent_all(0)
    pl.when(mid)(lambda: sent_all(1))
    pltpu.make_async_remote_copy(
        src_ref=lsev.at[0], dst_ref=lsev.at[1], send_sem=send_sem.at[2], recv_sem=one_recv.at[1],
        device_id=at_pair, device_id_type=MESH,
    ).wait_send()


def finish(dt_ref, ds_ref, src_t, dvf, dt_hbm, ds_hbm, dw_hbm, dw_ref, sems):
    small = [
        pltpu.make_async_copy(a, b, sems.at[n]) for n, (a, b) in enumerate(((dt_ref, dt_hbm), (ds_ref, ds_hbm)))
    ]
    for copy in small:
        copy.start()
    kw = dw_ref.shape[1]
    dv = jnp.concatenate(
        [dvf[a, b].reshape(-1, kw) for b in range(dvf.shape[1]) for a in range(CORES)], axis=0)
    pieces = 3
    tall = dw_ref.shape[0] // pieces
    for n in range(pieces):
        at = pl.ds(n * tall, tall)
        dw_ref[at] = dot(src_t[at], dv)
        copy = pltpu.make_async_copy(dw_ref.at[at], dw_hbm.at[at], sems.at[2 + n])
        copy.start()
        small.append(copy)
    for copy in small:
        copy.wait()


def finished(shape, dt, ds, src_t, dvf):
    vmem, hbm = pl.BlockSpec(memory_space=pltpu.VMEM), pl.BlockSpec(memory_space=pl.ANY)
    return pl.pallas_call(
        finish,
        out_shape=(
            jax.ShapeDtypeStruct(dt.shape, BF16), jax.ShapeDtypeStruct(ds.shape, BF16), jax.ShapeDtypeStruct(shape, F32),
        ),
        in_specs=[vmem] * 4,
        out_specs=(hbm,) * 3,
        scratch_shapes=[pltpu.VMEM(shape, F32), pltpu.SemaphoreType.DMA((5,))],
        compiler_params=pltpu.CompilerParams(vmem_limit_bytes=16 * 1024 * 1024),
    )(dt, ds, src_t, dvf)


def fused(sp, tp, queries, attn_out, log_norm, cotangent, keys, values, source, w_query, w_key, w_value):
    rows, model = queries.shape
    width = w_value.shape[0]
    rs, kw = keys.shape
    vmem, hbm = pl.BlockSpec(memory_space=pltpu.VMEM), pl.BlockSpec(memory_space=pl.ANY)
    dma = pltpu.SemaphoreType.DMA
    stack = (rows * HEADS // KV_HEADS, HEAD_DIM)
    half = model // KV_HEADS
    ny = sp // CORES
    scratch = [
        ((2, tp, sp * rs, HEAD_DIM), BF16), ((2, KV_HEADS, rs, HEAD_DIM), BF16),
        ((3, KV_HEADS) + stack, BF16), ((3,) + stack, BF16),
        (w_query.shape, BF16), (w_key.shape, BF16), (w_value.shape, BF16),
        (w_query.shape[::-1], BF16), (w_key.shape[::-1], BF16), (w_value.shape[::-1], BF16),
        ((CORES, ny) + source.shape, BF16),
        ((2, HEADS, rows), F32), ((2, stack[0], 128), F32), ((2, stack[0], 128), F32),
        ((2,) + stack, F32), ((rows, model), BF16), ((rows, half), BF16),
        ((2, sp * rs, HEAD_DIM), F32), ((2, stack[0], sp * rs), F32),
        ((2, sp, rs, HEAD_DIM), BF16), ((2, 3, rs, HEAD_DIM), BF16),
        ((tp, rs, kw), BF16), ((640,) + UNIT, BF16),
    ]
    return finished(w_value.shape, *pl.pallas_call(
        functools.partial(kernel, sp, tp),
        out_shape=(
            pltpu.VMEM((rows, width), BF16),
            pltpu.VMEM((source.shape[0], width), BF16),
            pltpu.VMEM((width, sp * source.shape[0]), BF16),
            pltpu.VMEM((CORES, ny, tp, rs, kw), BF16),
        ),
        in_specs=[hbm] * 10,
        out_specs=(vmem,) * 4,
        scratch_shapes=[pltpu.VMEM(s, t) for s, t in scratch] + [
            dma((8,)), dma((3,)), dma((tp, ny)), dma((tp, 2)), dma((tp,)), dma((11,)),
        ],
        compiler_params=pltpu.CompilerParams(
            collective_id=0, has_side_effects=True, vmem_limit_bytes=VMEM_BYTES
        ),
    )(log_norm.T, keys, values, queries, attn_out, cotangent, source, w_query, w_key, w_value))


def shards(sp, tp, *args):
    queries, keys, source = args[0], args[4], args[6]
    if sp == 2 * CORES and tp == 4 * SIDE and queries.shape[0] == 128 and sp * keys.shape[0] == 128 and source.shape[0] == 256:
        return fused(sp, tp, *args)
    return plain(*args)


def plain(queries, attn_out, log_norm, cotangent, keys, values, source, w_query, w_key, w_value):
    single_precision = jnp.float32
    repeat = HEADS // KV_HEADS
    score_scale = 1.0 / math.sqrt(HEAD_DIM)
    rows = queries.shape[0]
    near_keys, near_values = (
        lax.all_gather(keys, "sp", axis=0, tiled=True),
        lax.all_gather(values, "sp", axis=0, tiled=True),
    )
    span = near_keys.shape[0]
    query_tensor4 = queries.reshape(rows, KV_HEADS, repeat, HEAD_DIM)
    output_gradient4 = cotangent.reshape(rows, KV_HEADS, repeat, HEAD_DIM)
    out4 = attn_out.reshape(rows, KV_HEADS, repeat, HEAD_DIM)
    shared_key_heads = near_keys.reshape(span, KV_HEADS, HEAD_DIM)
    shared_value_heads = near_values.reshape(span, KV_HEADS, HEAD_DIM)
    delta = jnp.sum(
        output_gradient4.astype(single_precision) * out4.astype(single_precision), axis=3
    )
    delta = jnp.transpose(delta, (1, 2, 0))[..., None]
    lse = jnp.transpose(log_norm.reshape(rows, KV_HEADS, repeat), (1, 2, 0))[..., None]
    logit_scores = (
        jnp.einsum(
            "znjk,wnk->njzw",
            query_tensor4,
            shared_key_heads,
            preferred_element_type=single_precision,
        )
        * score_scale
    )
    probs = jnp.exp(logit_scores - lse)
    probabilities16 = probs.astype(jnp.bfloat16)
    prob_gradient = jnp.einsum(
        "znjk,wnk->njzw",
        output_gradient4,
        shared_value_heads,
        preferred_element_type=single_precision,
    )
    score_gradient = (probs * (prob_gradient - delta)).astype(jnp.bfloat16)
    query_gradient_piece = (
        jnp.einsum(
            "wohn,nwb->hwob",
            score_gradient,
            shared_key_heads,
            preferred_element_type=single_precision,
        )
        * score_scale
    )
    query_gradient_piece = query_gradient_piece.reshape(rows, -1)
    key_gradient_piece = (
        jnp.einsum(
            "nkjv,jnka->vna", score_gradient, query_tensor4, preferred_element_type=single_precision
        )
        * score_scale
    )
    value_gradient_piece = jnp.einsum(
        "nkjv,jnka->vna", probabilities16, output_gradient4, preferred_element_type=single_precision
    )
    own_keys, own_values = (
        lax.psum_scatter(
            key_gradient_piece.reshape(span, -1).astype(jnp.bfloat16),
            "sp",
            scatter_dimension=0,
            tiled=True,
        ).astype(jnp.float32),
        lax.psum_scatter(
            value_gradient_piece.reshape(span, -1).astype(jnp.bfloat16),
            "sp",
            scatter_dimension=0,
            tiled=True,
        ).astype(jnp.float32),
    )
    stacked = jnp.concatenate(
        [own_keys.astype(jnp.bfloat16), own_values.astype(jnp.bfloat16)], axis=1
    )
    group = lax.all_gather(stacked, "tp", axis=0, tiled=True)
    weights = jnp.concatenate([w_key, w_value], axis=1)
    d_source = lax.dot_general(
        group, weights, (((1,), (1,)), ((), ())), preferred_element_type=single_precision
    ).astype(jnp.bfloat16)
    kv_width = w_value.shape[1]
    weight_term = lax.dot_general(
        source,
        group[:, kv_width:],
        (((0,), (0,)), ((), ())),
        preferred_element_type=single_precision,
    )
    d_wvalue = lax.psum(weight_term.astype(jnp.bfloat16), "sp").astype(jnp.float32)
    dq16 = lax.psum(query_gradient_piece, "tp").astype(jnp.bfloat16)
    d_target = lax.dot_general(
        dq16, w_query, (((1,), (1,)), ((), ())), preferred_element_type=single_precision
    ).astype(jnp.bfloat16)
    return (d_target, d_source, d_wvalue)


def solution(mesh):
    body = functools.partial(shards, mesh.shape["sp"], mesh.shape["tp"])
    in_specs = (
        P("sp", None),
        P("sp", None),
        P("sp", None),
        P("sp", None),
        P(("sp", "tp"), None),
        P(("sp", "tp"), None),
        P("sp", "tp"),
        P("tp", None),
        P("tp", None),
        P("tp", None),
    )
    out_specs = (P("sp", "tp"), P("sp", "tp"), P("tp", None))
    return jax.shard_map(body, mesh=mesh, in_specs=in_specs, out_specs=out_specs, check_vma=False)
```

```python
import functools
import math

import jax
import jax.numpy as jnp
from jax import lax
from jax.experimental import pallas as pl
from jax.experimental.pallas import tpu as pltpu
from jax.sharding import PartitionSpec as P

HEADS = 12
KV_HEADS = 2
HEAD_DIM = 256
CORES = 2
SIDE = 2
VMEM_BYTES = 64880640
UNIT = (16, 256)
MESH = pl.DeviceIdType.MESH
NT = (((1,), (1,)), ((), ()))
TN = (((0,), (0,)), ((), ()))
F32 = jnp.float32
BF16 = jnp.bfloat16


def dot(a, b, dims=(((1,), (0,)), ((), ()))):
    return lax.dot_general(a, b, dims, preferred_element_type=F32)


def kernel(
    sp, tp, lse_hbm, k_hbm, v_hbm, q_hbm, o_hbm, do_hbm, src_hbm, wq_hbm, wk_hbm, wv_hbm,
    dt_ref, ds_ref, src_t, dvf,
    kv, kvs, att, attr, wq, wk, wv, wqt, wkt, wvt, src, lsev, lse, delta, dqa, dq16, dqs, acc, prob,
    part, got, dkf, units,
    load_sem, send_sem, kv_recv, g_recv, gy_recv, one_recv,
):
    rows = q_hbm.shape[0]
    rs, kw = k_hbm.shape
    repeat = HEADS // KV_HEADS
    scale = 1.0 / math.sqrt(HEAD_DIM)
    log2e = math.log2(math.e)
    unit = UNIT[0] * UNIT[1] * 2
    i, j = lax.axis_index("sp"), lax.axis_index("tp")
    nz = tp // SIDE
    y, c = i // CORES, lax.rem(i, CORES)
    z, x = j // SIDE, lax.rem(j, SIDE)
    oy, oc, ox = 1 - y, 1 - c, 1 - x
    orders = [sorted((b for b in range(nz) if b != a), key=lambda b, a=a: abs(a - b)) for a in range(nz)]
    zs = [sum(jnp.where(z == a, order[n], 0) for a, order in enumerate(orders)) for n in range(nz - 1)]
    mid = (z == 1) | (z == 2)
    edge = jnp.where(z == 1, 0, 3)
    jx = z * SIDE + ox
    mine = [a * SIDE + x for a in zs]
    far = [a * SIDE + ox for a in zs]
    at_pair = (y * CORES + oc, j)
    at_y = (oy * CORES + c, j)
    at_x = (i, jx)
    sent = [0, 0]

    def bytes_of(ref):
        return math.prod(ref.shape) * jnp.dtype(ref.dtype).itemsize

    def send(a, b, r, device, s=0):
        pltpu.make_async_remote_copy(
            src_ref=a, dst_ref=b, send_sem=send_sem.at[s % 3], recv_sem=r, device_id=device, device_id_type=MESH,
        ).start()
        if s < 2:
            sent[s] += bytes_of(a)

    def receive(ref, r):
        pltpu.make_async_remote_copy(
            src_ref=ref, dst_ref=ref, send_sem=send_sem.at[0], recv_sem=r, device_id=at_pair, device_id_type=MESH,
        ).wait_recv()

    def load(a, b, s):
        pltpu.make_async_copy(a, b, load_sem.at[s]).start()
        return bytes_of(b)

    def take(size, s):
        ref = units.at[pl.ds(0, size // unit)]
        pltpu.make_async_copy(ref, ref, load_sem.at[s]).wait()

    own = pl.ds(pl.multiple_of(i * rs, rs), rs)
    theirs = pl.ds(pl.multiple_of((y * CORES + oc) * rs, rs), rs)
    kv_size = 0
    for t, r in enumerate((k_hbm, v_hbm)):
        for g in range(KV_HEADS):
            kv_size += load(r.at[:, pl.ds(g * HEAD_DIM, HEAD_DIM)], kvs.at[t, g], 0)
        kv_size += load(r.at[:, pl.ds(pl.multiple_of(c * HEAD_DIM, HEAD_DIM), HEAD_DIM)], kv.at[t, j, own], 0)
    barrier = pltpu.get_barrier_semaphore()

    def signal(device):
        pl.semaphore_signal(barrier, inc=1, device_id=device, device_id_type=MESH)

    near = [at_pair]
    for g in range(CORES):
        near += [(oy * CORES + g, j), (y * CORES + g, jx), (y * CORES + g, mine[0]), (y * CORES + g, mine[1])]
    for d in near:
        signal(d)

    @pl.when(mid)
    def _():
        for g in range(CORES):
            signal((y * CORES + g, mine[2]))

    def load_heads(g, a, r, s):
        size = 0
        for h in range(repeat):
            columns = pl.ds(pl.multiple_of((g * repeat + h) * HEAD_DIM, HEAD_DIM), HEAD_DIM)
            size += load(r.at[:, columns], att.at[a, g, pl.ds(h * rows, rows)], s)
        return size

    attn = (q_hbm, do_hbm, o_hbm)
    head_size = [load_heads(oc, a, r, 1 + a) for a, r in enumerate(attn)][0]
    own_size = sum(load_heads(c, a, r, 4) for a, r in enumerate(attn))
    load(lse_hbm, lsev.at[0], 5)
    src_size = load(src_hbm, src.at[c, y], 6)
    weight_size = load(wk_hbm, wk, 7) + load(wv_hbm, wv, 7)
    weight_size += load(wq_hbm, wq, 7)
    take(kv_size, 0)
    pl.semaphore_wait(barrier, len(near) + 2 * mid.astype(jnp.int32))


    def raw(y_to, slot, s=0):
        for g in range(CORES):
            send(kvs.at[:, g], kv.at[:, j, own], kv_recv.at[j, y], (y_to * CORES + g, slot), s)

    for t in range(2):
        for g in range(CORES):
            to = (oy * CORES + g, j)
            send(kvs.at[t, g], kv.at[t, j, own], kv_recv.at[j, y] if t == 0 else one_recv.at[9], to)
        send(kvs.at[t, oc], kv.at[t, j, own], kv_recv.at[j, y] if t == 0 else one_recv.at[10], at_pair)
    raw(y, jx)
    raw(y, mine[0])
    raw(y, mine[1])

    @pl.when(mid)
    def _():
        raw(y, mine[2], 1)

    def src_send(first):
        ref = src.at[c, y, pl.ds(0, cut) if first else pl.ds(cut, src.shape[2] - cut)]
        send(ref, ref, one_recv.at[3], at_y)

    cut = src.shape[2] * 5 // 8
    for a in range(3):
        take(head_size, 1 + a)
        send(att.at[a, oc], attr.at[a], one_recv.at[0 if a < 2 else 7], at_pair)
    pltpu.make_async_copy(lse_hbm, lsev.at[0], load_sem.at[5]).wait()
    send(lsev.at[0], lsev.at[1], one_recv.at[1], at_pair, 2)
    take(own_size, 4)
    take(src_size, 6)
    src_send(True)
    send(src.at[c, y], src.at[c, y], one_recv.at[4], at_pair)

    def block(b, a):
        return att[a, c] if b == 0 else attr[a]

    def deltas(b):
        for h in range(repeat):
            at = pl.ds(h * rows, rows)
            do, o = (att[a, c, at] if b == 0 else attr[a, at] for a in (1, 2))
            d = jnp.sum(do.astype(F32) * o.astype(F32), axis=1, keepdims=True)
            delta[b, at] = jnp.broadcast_to(d, (rows, 128))

    def norms(b):
        for h in range(repeat):
            row = jnp.where(c == 0, lsev[b, h:h + 1, :], lsev[b, repeat + h:repeat + h + 1, :])
            lse[b, pl.ds(h * rows, rows)] = jnp.transpose(jnp.broadcast_to(row * log2e, (128, rows)))

    norms(0)
    deltas(0)
    take(weight_size, 7)
    for n in range(repeat):
        columns = slice(n * kw, (n + 1) * kw)
        wqt[columns, :] = jnp.transpose(wq[:, columns])
    wkt[...] = jnp.transpose(wk[...])
    wvt[...] = jnp.transpose(wv[...])

    def piece(slot, h):
        return kv.at[:, slot, pl.ds(pl.multiple_of(h * (CORES * rs), CORES * rs), CORES * rs)]

    def arrived(slot, h):
        receive(piece(slot, h), kv_recv.at[slot, h])

    def relay(slot, h, device, s=0):
        send(piece(slot, h), piece(slot, h), kv_recv.at[slot, h], device, s)

    def from_z(n, h, s=0):
        arrived(mine[n], h)
        relay(mine[n], h, at_x, s)

    def half_piece(t):
        return kv.at[t, j, pl.ds(pl.multiple_of(oy * (CORES * rs), CORES * rs), CORES * rs)]

    def along_z(t):
        def one(device, s=0):
            send(half_piece(t), half_piece(t), kv_recv.at[j, oy], device, s)

        one((i, mine[0]))
        one(at_x)

        @pl.when(mid)
        def _():
            one((i, mine[1]), 1)
            one((i, mine[2]), 1)

    receive(kv.at[0, j, theirs], kv_recv.at[j, y])
    receive(half_piece(0), kv_recv.at[j, oy])
    along_z(0)
    receive(attr.at[pl.ds(0, 2)], one_recv.at[0])
    receive(lsev.at[1], one_recv.at[1])
    norms(1)

    def wide(a, n):
        return a if n == 1 else jnp.concatenate([a] * n, axis=1)

    def probs(b, keys):
        return jnp.exp2(dot(block(b, 0), keys, NT) * (scale * log2e) - wide(lse[b], keys.shape[0] // 128))

    def scores(b, p, values):
        dp = dot(block(b, 1), values, NT)
        return (p * (dp - wide(delta[b], values.shape[0] // 128))).astype(BF16)

    def part_send(t, r):
        for g in range(CORES):
            to = oy * CORES + g
            send(part.at[t, to], got.at[t, 1 + c], r, (to, j))
        send(part.at[t, y * CORES + oc], got.at[t, 0], r, at_pair)

    for b in range(2):
        p = probs(b, kv[0, j])
        prob[b] = p
        dv = dot(p.astype(BF16), block(b, 1), TN)
        if b == 0:
            acc[1] = dv
        else:
            part[1] = (acc[1] + dv).astype(BF16).reshape(sp, rs, HEAD_DIM)
    part_send(1, one_recv.at[2])
    receive(kv.at[1, j, theirs], one_recv.at[10])
    receive(half_piece(1), one_recv.at[9])
    along_z(1)
    from_z(0, y)
    receive(attr.at[2], one_recv.at[7])
    deltas(1)
    for b in range(2):
        keys = kv[0, j]
        ds = scores(b, prob[b], kv[1, j])
        dk = dot(ds, block(b, 0), TN)
        dqa[b] = dot(ds, keys)
        if b == 0:
            acc[0] = dk

            @pl.when(mid)
            def _():
                arrived(mine[1], y)
                relay(mine[1], y, at_x, 3)
                arrived(mine[2], y)
                relay(mine[2], y, (i, edge * SIDE + x), 1)
                relay(mine[2], y, at_y, 3)

        else:
            part[0] = ((acc[0] + dk) * scale).astype(BF16).reshape(sp, rs, HEAD_DIM)
    part_send(0, one_recv.at[8])
    src_send(False)

    def chunk(slots, order=(0, 1)):
        for b in order:
            keys, values = (kv[t, slots].reshape(-1, HEAD_DIM) for t in range(2))
            dqa[b] += dot(scores(b, probs(b, keys), values), keys)

    def total(t):
        here = part[t, i].astype(F32) + got[t, 1 + c].astype(F32)
        there = got[t, 0].astype(F32) + got[t, 1 + oc].astype(F32)
        ref = dkf.at[j] if t == 0 else dvf.at[c, y, j]
        for g in range(KV_HEADS):
            ref[:, g * HEAD_DIM:(g + 1) * HEAD_DIM] = jnp.where(c == g, here, there).astype(BF16)

    def grad(t, slot):
        return dkf.at[slot] if t == 0 else dvf.at[c, y, slot]

    def g_send(t, slot, device, s=0):
        send(grad(t, slot), grad(t, slot), g_recv.at[slot, t], device, s)

    def g_arrived(t, slot):
        receive(grad(t, slot), g_recv.at[slot, t])

    def g_along_z(t, slot):
        pl.when(mid)(lambda: g_send(t, slot, (i, mine[2]), 1 if t == 1 else 3))
        g_send(t, slot, (i, mine[1]))
        g_send(t, slot, (i, mine[0]))
        if t == 0:
            sent[0] += bytes_of(grad(t, slot))

    def g_spread(slot, last=False, s=0):
        ref = grad(1, slot)
        send(ref, ref, gy_recv.at[slot], at_y, s)
        send(ref, ref, one_recv.at[5], at_pair, s)
        if last:
            send(ref, ref, one_recv.at[5], (oy * CORES + oc, j), s)

    def g_from_y(slot, last=False):
        ref = dvf.at[c, oy, slot]
        receive(ref, gy_recv.at[slot])
        if not last:
            send(ref, ref, one_recv.at[5], at_pair)

    def dv_from(slot):
        g_arrived(1, slot)
        g_spread(slot)

    def dv_last(slot, early, last=False):
        def body():
            g_arrived(1, slot)
            if early:
                g_send(1, slot, (i, edge * SIDE + x), 1)
            g_spread(slot, last, 0 if early else 3)

        pl.when(mid if early else jnp.logical_not(mid))(body)

    def dk_from(n):
        g_arrived(0, mine[n])
        g_send(0, mine[n], at_x)

    def chunk_z(n, order=(0, 1)):
        chunk(pl.ds(zs[n] * SIDE, SIDE), order)

    def far_arrived(n):
        arrived(far[n], y)
        arrived(far[n], oy)

    receive(got.at[1], one_recv.at[2])
    total(1)
    g_send(1, j, at_x)
    g_along_z(1, j)
    g_spread(j)

    @pl.when(mid)
    def _():
        relay(mine[2], y, at_x, 3)

    @pl.when(jnp.logical_not(mid))
    def _():
        arrived(mine[1], y)
        relay(mine[1], y, at_x)

    sent[0] += 2 * bytes_of(piece(mine[2], y))
    from_z(0, oy)
    pl.when(mid)(lambda: from_z(2, oy, 3))
    arrived(jx, y)
    arrived(jx, oy)
    chunk(pl.ds(jx, 1))
    receive(got.at[0], one_recv.at[8])
    total(0)
    g_along_z(0, j)
    pl.when(jnp.logical_not(mid))(lambda: g_send(0, j, (i, mine[2]), 3))
    g_send(0, j, at_x)
    from_z(1, oy)
    g_arrived(1, jx)
    g_along_z(1, jx)
    g_spread(jx)

    @pl.when(jnp.logical_not(mid))
    def _():
        arrived(mine[2], y)
        relay(mine[2], y, at_y, 3)
        relay(mine[2], y, at_x, 3)

    dv_from(mine[0])
    dv_last(mine[2], True)
    far_arrived(0)
    chunk_z(0)
    pl.when(jnp.logical_not(mid))(lambda: from_z(2, oy))
    dv_from(mine[1])
    dv_from(far[0])
    dv_last(far[2], True, True)
    receive(src.at[c, oy], one_recv.at[3])
    send(src.at[c, oy], src.at[c, oy], one_recv.at[4], at_pair)
    far_arrived(1)
    chunk_z(1)
    dv_last(mine[2], False)
    dk_from(0)
    dk_from(1)
    g_from_y(j)
    g_from_y(jx)
    dv_from(far[1])
    dk_from(2)
    receive(src.at[oc], one_recv.at[4])
    deep = src.shape[2]
    for b in range(sp // CORES):
        for a in range(CORES):
            n = b * CORES + a
            src_t[:, n * deep:(n + 1) * deep] = jnp.transpose(src[a, b])
    far_arrived(2)
    dv_last(far[2], False, True)
    chunk_z(2, (1,))

    def rounded(b, ref):
        for h in range(repeat):
            ref[:, h * HEAD_DIM:(h + 1) * HEAD_DIM] = (dqa[b, h * rows:(h + 1) * rows] * scale).astype(BF16)

    half = dqs.shape[1]
    rounded(1, dqs)
    send(dqs, dq16.at[:, pl.ds(pl.multiple_of(c * half, half), half)], one_recv.at[6], at_pair)
    chunk_z(2, (0,))
    for h in range(repeat):
        at = pl.ds(pl.multiple_of(c * half + h * HEAD_DIM, HEAD_DIM), HEAD_DIM)
        dq16[:, at] = (dqa[0, h * rows:(h + 1) * rows] * scale).astype(BF16)
    for slot in [mine[0], mine[1], far[0], mine[2], far[1]]:
        g_from_y(slot)
    receive(dq16.at[:, pl.ds(pl.multiple_of(oc * half, half), half)], one_recv.at[6])
    dt_ref[...] = dot(dq16[...], wqt[...]).astype(BF16)
    g_arrived(0, jx)
    for n in range(nz - 1):
        g_arrived(0, far[n])
    ds_ref[...] = (
        dot(dkf[...].reshape(-1, kw), wkt[...]) + dot(dvf[c, y].reshape(-1, kw), wvt[...])
    ).astype(BF16)
    g_from_y(far[2], True)
    receive(dvf.at[oc], one_recv.at[5])

    def sent_all(s):
        ref = units.at[pl.ds(0, sent[s] // unit)]
        pltpu.make_async_remote_copy(
            src_ref=ref, dst_ref=ref, send_sem=send_sem.at[s], recv_sem=one_recv.at[0],
            device_id=at_pair, device_id_type=MESH,
        ).wait_send()

    sent_all(0)
    pl.when(mid)(lambda: sent_all(1))
    pltpu.make_async_remote_copy(
        src_ref=lsev.at[0], dst_ref=lsev.at[1], send_sem=send_sem.at[2], recv_sem=one_recv.at[1],
        device_id=at_pair, device_id_type=MESH,
    ).wait_send()


def finish(dt_ref, ds_ref, src_t, dvf, dt_hbm, ds_hbm, dw_hbm, dw_ref, sems):
    small = [
        pltpu.make_async_copy(a, b, sems.at[n]) for n, (a, b) in enumerate(((dt_ref, dt_hbm), (ds_ref, ds_hbm)))
    ]
    for copy in small:
        copy.start()
    kw = dw_ref.shape[1]
    dv = jnp.concatenate(
        [dvf[a, b].reshape(-1, kw) for b in range(dvf.shape[1]) for a in range(CORES)], axis=0)
    pieces = 3
    tall = dw_ref.shape[0] // pieces
    for n in range(pieces):
        at = pl.ds(n * tall, tall)
        dw_ref[at] = dot(src_t[at], dv)
        copy = pltpu.make_async_copy(dw_ref.at[at], dw_hbm.at[at], sems.at[2 + n])
        copy.start()
        small.append(copy)
    for copy in small:
        copy.wait()


def finished(shape, dt, ds, src_t, dvf):
    vmem, hbm = pl.BlockSpec(memory_space=pltpu.VMEM), pl.BlockSpec(memory_space=pl.ANY)
    return pl.pallas_call(
        finish,
        out_shape=(
            jax.ShapeDtypeStruct(dt.shape, BF16), jax.ShapeDtypeStruct(ds.shape, BF16), jax.ShapeDtypeStruct(shape, F32),
        ),
        in_specs=[vmem] * 4,
        out_specs=(hbm,) * 3,
        scratch_shapes=[pltpu.VMEM(shape, F32), pltpu.SemaphoreType.DMA((5,))],
        compiler_params=pltpu.CompilerParams(vmem_limit_bytes=16 * 1024 * 1024),
    )(dt, ds, src_t, dvf)


def fused(sp, tp, queries, attn_out, log_norm, cotangent, keys, values, source, w_query, w_key, w_value):
    rows, model = queries.shape
    width = w_value.shape[0]
    rs, kw = keys.shape
    vmem, hbm = pl.BlockSpec(memory_space=pltpu.VMEM), pl.BlockSpec(memory_space=pl.ANY)
    dma = pltpu.SemaphoreType.DMA
    stack = (rows * HEADS // KV_HEADS, HEAD_DIM)
    half = model // KV_HEADS
    ny = sp // CORES
    scratch = [
        ((2, tp, sp * rs, HEAD_DIM), BF16), ((2, KV_HEADS, rs, HEAD_DIM), BF16),
        ((3, KV_HEADS) + stack, BF16), ((3,) + stack, BF16),
        (w_query.shape, BF16), (w_key.shape, BF16), (w_value.shape, BF16),
        (w_query.shape[::-1], BF16), (w_key.shape[::-1], BF16), (w_value.shape[::-1], BF16),
        ((CORES, ny) + source.shape, BF16),
        ((2, HEADS, rows), F32), ((2, stack[0], 128), F32), ((2, stack[0], 128), F32),
        ((2,) + stack, F32), ((rows, model), BF16), ((rows, half), BF16),
        ((2, sp * rs, HEAD_DIM), F32), ((2, stack[0], sp * rs), F32),
        ((2, sp, rs, HEAD_DIM), BF16), ((2, 3, rs, HEAD_DIM), BF16),
        ((tp, rs, kw), BF16), ((640,) + UNIT, BF16),
    ]
    return finished(w_value.shape, *pl.pallas_call(
        functools.partial(kernel, sp, tp),
        out_shape=(
            pltpu.VMEM((rows, width), BF16),
            pltpu.VMEM((source.shape[0], width), BF16),
            pltpu.VMEM((width, sp * source.shape[0]), BF16),
            pltpu.VMEM((CORES, ny, tp, rs, kw), BF16),
        ),
        in_specs=[hbm] * 10,
        out_specs=(vmem,) * 4,
        scratch_shapes=[pltpu.VMEM(s, t) for s, t in scratch] + [
            dma((8,)), dma((3,)), dma((tp, ny)), dma((tp, 2)), dma((tp,)), dma((11,)),
        ],
        compiler_params=pltpu.CompilerParams(
            collective_id=0, has_side_effects=True, vmem_limit_bytes=VMEM_BYTES
        ),
    )(log_norm.T, keys, values, queries, attn_out, cotangent, source, w_query, w_key, w_value))


def shards(sp, tp, *args):
    queries, keys, source = args[0], args[4], args[6]
    if sp == 2 * CORES and tp == 4 * SIDE and queries.shape[0] == 128 and sp * keys.shape[0] == 128 and source.shape[0] == 256:
        return fused(sp, tp, *args)
    return plain(*args)


def plain(queries, attn_out, log_norm, cotangent, keys, values, source, w_query, w_key, w_value):
    single_precision = jnp.float32
    repeat = HEADS // KV_HEADS
    score_scale = 1.0 / math.sqrt(HEAD_DIM)
    rows = queries.shape[0]
    near_keys, near_values = (
        lax.all_gather(keys, "sp", axis=0, tiled=True),
        lax.all_gather(values, "sp", axis=0, tiled=True),
    )
    span = near_keys.shape[0]
    query_tensor4 = queries.reshape(rows, KV_HEADS, repeat, HEAD_DIM)
    output_gradient4 = cotangent.reshape(rows, KV_HEADS, repeat, HEAD_DIM)
    out4 = attn_out.reshape(rows, KV_HEADS, repeat, HEAD_DIM)
    shared_key_heads = near_keys.reshape(span, KV_HEADS, HEAD_DIM)
    shared_value_heads = near_values.reshape(span, KV_HEADS, HEAD_DIM)
    delta = jnp.sum(
        output_gradient4.astype(single_precision) * out4.astype(single_precision), axis=3
    )
    delta = jnp.transpose(delta, (1, 2, 0))[..., None]
    lse = jnp.transpose(log_norm.reshape(rows, KV_HEADS, repeat), (1, 2, 0))[..., None]
    logit_scores = (
        jnp.einsum(
            "znjk,wnk->njzw",
            query_tensor4,
            shared_key_heads,
            preferred_element_type=single_precision,
        )
        * score_scale
    )
    probs = jnp.exp(logit_scores - lse)
    probabilities16 = probs.astype(jnp.bfloat16)
    prob_gradient = jnp.einsum(
        "znjk,wnk->njzw",
        output_gradient4,
        shared_value_heads,
        preferred_element_type=single_precision,
    )
    score_gradient = (probs * (prob_gradient - delta)).astype(jnp.bfloat16)
    query_gradient_piece = (
        jnp.einsum(
            "wohn,nwb->hwob",
            score_gradient,
            shared_key_heads,
            preferred_element_type=single_precision,
        )
        * score_scale
    )
    query_gradient_piece = query_gradient_piece.reshape(rows, -1)
    key_gradient_piece = (
        jnp.einsum(
            "nkjv,jnka->vna", score_gradient, query_tensor4, preferred_element_type=single_precision
        )
        * score_scale
    )
    value_gradient_piece = jnp.einsum(
        "nkjv,jnka->vna", probabilities16, output_gradient4, preferred_element_type=single_precision
    )
    own_keys, own_values = (
        lax.psum_scatter(
            key_gradient_piece.reshape(span, -1).astype(jnp.bfloat16),
            "sp",
            scatter_dimension=0,
            tiled=True,
        ).astype(jnp.float32),
        lax.psum_scatter(
            value_gradient_piece.reshape(span, -1).astype(jnp.bfloat16),
            "sp",
            scatter_dimension=0,
            tiled=True,
        ).astype(jnp.float32),
    )
    stacked = jnp.concatenate(
        [own_keys.astype(jnp.bfloat16), own_values.astype(jnp.bfloat16)], axis=1
    )
    group = lax.all_gather(stacked, "tp", axis=0, tiled=True)
    weights = jnp.concatenate([w_key, w_value], axis=1)
    d_source = lax.dot_general(
        group, weights, (((1,), (1,)), ((), ())), preferred_element_type=single_precision
    ).astype(jnp.bfloat16)
    kv_width = w_value.shape[1]
    weight_term = lax.dot_general(
        source,
        group[:, kv_width:],
        (((0,), (0,)), ((), ())),
        preferred_element_type=single_precision,
    )
    d_wvalue = lax.psum(weight_term.astype(jnp.bfloat16), "sp").astype(jnp.float32)
    dq16 = lax.psum(query_gradient_piece, "tp").astype(jnp.bfloat16)
    d_target = lax.dot_general(
        dq16, w_query, (((1,), (1,)), ((), ())), preferred_element_type=single_precision
    ).astype(jnp.bfloat16)
    return (d_target, d_source, d_wvalue)


def solution(mesh):
    body = functools.partial(shards, mesh.shape["sp"], mesh.shape["tp"])
    in_specs = (
        P("sp", None),
        P("sp", None),
        P("sp", None),
        P("sp", None),
        P(("sp", "tp"), None),
        P(("sp", "tp"), None),
        P("sp", "tp"),
        P("tp", None),
        P("tp", None),
        P("tp", None),
    )
    out_specs = (P("sp", "tp"), P("sp", "tp"), P("tp", None))
    return jax.shard_map(body, mesh=mesh, in_specs=in_specs, out_specs=out_specs, check_vma=False)
```
